128 devices in a mesh: sp: 16 (over z, y), tp: 8 (over x, core).
Axes of the slice: x: 4, y: 4, z: 4, core: 2. Of those that a mesh axis runs over, the one named last changes fastest.
Arguments:
- stream: bfloat16 [32768, 4096], P('sp', 'tp'), may hold values from -18 to 18
- doc_ids: int32 [32768], P('sp'), may hold values from 0 to 3, never falling along the last dimension, each value on 1 to 12288 neighbouring positions
- norm_gain: bfloat16 [3, 4096], replicated, may hold values from 0.099609375 to 1.8984375
- proj_in: bfloat16 [3, 4096, 1024], P(None, 'tp', 'sp'), may hold values from -0.09375 to 0.09375
- mix_pool: bfloat16 [3, 8, 128, 128], replicated, may hold values from -0.5 to 0.5
- pool_gain: bfloat16 [3, 1024], replicated, may hold values from 0.099609375 to 1.8984375
- proj_out: bfloat16 [3, 1024, 4096], P(None, 'sp', 'tp'), may hold values from -0.1875 to 0.1875
Outputs:
- stream_out: bfloat16 [32768, 4096], P('sp', 'tp')
The draws below stay inside these ranges and needn't reach their ends.
Inputs may be any that keep to these rules, and one draw needn't show every extreme that they name: `doc_ids`: document numbers never fall along the sequence; each document holds 1 to 12288 positions, one exactly that many.
All inputs are finite; a program needn't handle non-finite values.
Results may differ from the reference program's by a relative error of at most 0.02.
Values may be sent and summed in bfloat16 or wider, within the bound.
A program may use at most 64 MiB of HBM per device.

```python
import math
import jax
import jax.numpy as jnp
import numpy as np
from jax import lax

D = 4096
POOL = 1024
GROUP = 128
LAYERS = 3
TOK = 2048
GROUPS = 8
TOKENS = 32768
DOCS = 4
N_TP = 8


def draw_stream(key, part):
    key_base = jax.random.fold_in(key, 11)
    key_cols = jax.random.fold_in(key, 12)
    column_scale = jnp.exp(jax.random.uniform(key_cols, (32,), jnp.float32, -1.1, 1.1))
    column_scale = jnp.repeat(column_scale, D // 32)
    base = jnp.clip(jax.random.normal(key_base, (TOKENS, D), jnp.float32), -6.0, 6.0)
    values = jnp.clip(base * column_scale[None, :], -18.0, 18.0)
    return values.astype(jnp.bfloat16)


def block_scale(own_key, shape, pieces, low, high):
    level, own = 1.0, jax.random.fold_in(own_key, 6)
    for position, blocks in pieces:
        steps = jnp.exp(jax.random.uniform(jax.random.fold_in(own, position), (blocks,), jnp.float32, low / len(pieces), high / len(pieces)))
        level = level * jnp.repeat(steps, shape[position] // blocks).reshape([-1 if axis == position else 1 for axis in range(len(shape))])
    return level


def split_up(count, total, limit, lean):
    portions = [(1 << 20) // math.isqrt(rank ** lean) + 1 for rank in range(2, count + 1)]
    spare, given = total - limit - (count - 1), [1] * (count - 1)
    while spare > 0:
        movable = [i for i in range(count - 1) if given[i] < limit]
        whole, left = sum([portions[i] for i in movable]), spare
        for i in movable:
            more = min(limit - given[i], max(1, left * portions[i] // whole), spare)
            given[i] = given[i] + more
            spare = spare - more
    return np.array([limit] + given)


def ragged(rng, count, total, limit, slope):
    if count == 2:
        one = jax.random.randint(rng, (), max(1, total - limit), min(limit, total - 1) + 1)
        return jnp.stack([one, total - one])
    lengths = jnp.asarray(split_up(count, total, limit, slope), jnp.int32)
    twos = (count - 1) // 2
    source_of, receiver = lengths[1:1 + 2 * twos:2], lengths[2:2 + 2 * twos:2]
    room = jnp.minimum(source_of - 1, limit - receiver)
    passed = jax.random.randint(jax.random.fold_in(rng, 1), (twos,), 0, 1 << 20) % (room + 1)
    lengths = lengths.at[1:1 + 2 * twos:2].set(source_of - passed).at[2:2 + 2 * twos:2].set(receiver + passed)
    return lengths[jax.random.permutation(jax.random.fold_in(rng, 2), count)]


def normal_values(rng, dims, deviation, bound, shards=(), held_as=jnp.bfloat16):
    entries = jax.random.normal(rng, dims, jnp.float32) * deviation
    if len(shards) > 0:
        entries = block_scale(rng, dims, shards, -0.22, 0.18) * entries
    return jnp.clip(entries, min=-bound, max=bound).astype(held_as)


def setup_inputs(seed: int = 0) -> dict:
    key_of = jax.random.split(jax.random.key(seed), 8)
    return {
        "stream": draw_stream(jax.random.fold_in(key_of[7], 71), 0),
        "doc_ids": jnp.searchsorted(jnp.cumsum(ragged(key_of[1], DOCS, TOKENS, 6 * TOK, 1)), jnp.arange(TOKENS), side="right").astype(jnp.int32),
        "norm_gain": jnp.clip(1.0 + 0.18 * jax.random.normal(key_of[2], (LAYERS, D), jnp.float32), 0.099609375, 1.8984375).astype(jnp.bfloat16),
        "proj_in": normal_values(key_of[3], (LAYERS, D, POOL), D ** -0.5, 0.09375, ((1, 8), (2, 16))),
        "mix_pool": normal_values(key_of[4], (LAYERS, GROUPS, GROUP, GROUP), GROUP ** -0.5, 0.5),
        "pool_gain": jnp.clip(1.0 + 0.18 * jax.random.normal(key_of[5], (LAYERS, POOL), jnp.float32), 0.099609375, 1.8984375).astype(jnp.bfloat16),
        "proj_out": normal_values(key_of[6], (LAYERS, POOL, D), POOL ** -0.5, 0.1875, ((1, 16), (2, 8))),
    }


epsilon = 1e-06
span_reach = 15

def span_pool(padded, labels, widths):
    kept = padded.shape[0] - span_reach
    own_label = labels[span_reach:]
    summed = jnp.zeros((kept, padded.shape[1]), jnp.float32)
    counted = jnp.zeros((kept, padded.shape[1]), jnp.float32)
    for offset in range(span_reach + 1):
        first = span_reach - offset
        member = (labels[first:first + kept] == own_label)[:, None] & (offset < widths)[None, :]
        factor = member.astype(jnp.float32)
        summed = summed + padded[first:first + kept] * factor
        counted = counted + factor
    return summed / counted - padded[span_reach:]

def reference(stream, doc_ids, norm_gain, proj_in, mix_pool, pool_gain, proj_out):
    hidden = stream
    labels = (doc_ids + 1).astype(jnp.int32)
    tags = jnp.concatenate([jnp.zeros((span_reach,), jnp.int32), labels])
    channel = jnp.arange(POOL, dtype=jnp.int32)
    widths = jnp.left_shift(jnp.int32(2), channel // GROUP % 4)
    block = D // N_TP
    for layer in range(LAYERS):
        wide = hidden.astype(jnp.float32)
        scale_rows = lax.rsqrt(lax.optimization_barrier(jnp.mean(wide * wide, axis=1)) + epsilon)
        gained = (wide * norm_gain[layer].astype(jnp.float32)[None, :]).astype(jnp.bfloat16)
        summed_in = jnp.zeros((hidden.shape[0], POOL), jnp.float32)
        for piece in range(N_TP):
            partial_value = jnp.dot(gained[:, piece * block:(piece + 1) * block], proj_in[layer, piece * block:(piece + 1) * block], preferred_element_type=jnp.float32)
            summed_in = summed_in + lax.optimization_barrier(partial_value.astype(jnp.bfloat16)).astype(jnp.float32)
        mixed_in = (summed_in * scale_rows[:, None]).astype(jnp.bfloat16)
        padded = jnp.concatenate([jnp.zeros((span_reach, POOL), jnp.float32), mixed_in.astype(jnp.float32)])
        pooled = span_pool(padded, tags, widths).astype(jnp.bfloat16)
        grouped = pooled.reshape(hidden.shape[0], GROUPS, GROUP).astype(jnp.float32)
        blended = jnp.einsum('tgc,gcd->tgd', grouped, mix_pool[layer].astype(jnp.float32)).reshape(hidden.shape[0], POOL)
        mixed = (blended * pool_gain[layer].astype(jnp.float32)[None, :]).astype(jnp.bfloat16)
        update = jnp.dot(mixed, proj_out[layer], preferred_element_type=jnp.float32)
        hidden = (wide + update).astype(jnp.bfloat16)
    return hidden
```

```python
import jax
import jax.numpy as jnp
from jax import lax
from jax.experimental import pallas as pl
from jax.experimental.pallas import tpu as pltpu
from jax.sharding import PartitionSpec as P

MESH = pl.DeviceIdType.MESH
F32 = jnp.float32
BF16 = jnp.bfloat16

D = 4096
POOL = 1024
GROUP = 128
GROUPS = POOL // GROUP
LAYERS = 3
MATS = 2 * LAYERS
TOK = 2048
COLS = 512
PART = TOK // 4
WIDE = 4 * COLS
HALO = 48
LEAD = 16
CHUNKS = 5
CH = (HALO + PART) // CHUNKS
WINDOWS = (2, 4, 8, 16)
EPS = 1e-06


def kernel(
    stream, docs, norm_gain, w_in, mix_pool, pool_gain, out,
    wbuf, hbuf, own, got, ssown, ssgot, gbuf, zbuf, mbuf, sqbuf, band, inv, ext,
    loc_w, loc_h, loc_hh, loc_o,
    s0, r0, s1, r1, s1f, r1f, s2, r2, s2f, r2f, s3, r3,
    sh, rh, shh, rhh, sl, rl, sx, rx, sq, rq, so, ro,
):
    sp = lax.axis_index("sp")
    tp = lax.axis_index("tp")
    z, y = sp // 4, sp % 4
    x, core = tp // 2, tp % 2
    half, xl = x // 2, x % 2
    me = xl * 2 + core
    mine = (me + 2 * half) % 4

    def remote(src, dst, send, recv, device):
        return pltpu.make_async_remote_copy(
            src_ref=src, dst_ref=dst, send_sem=send, recv_sem=recv,
            device_id=device, device_id_type=MESH,
        )

    across = (sp, (2 * half + 1 - xl) * 2 + core)
    partner = (sp, (3 - x) * 2 + core)
    sibling = (sp, x * 2 + 1 - core)

    def along_y(d):
        return (z * 4 + (y + d + 4) % 4, tp)

    def along_z(d):
        return (((z + d + 4) % 4) * 4 + y, tp)

    first_axis = (along_y, along_z)
    second_axis = (along_z, along_y)
    steps = (1, -1)

    def shard(m, k, d):
        if k == 0:
            return wbuf.at[m, core, 0, z, (y + d + 4) % 4]
        return wbuf.at[m, core, 1, (z + d + 4) % 4, y]

    def plane(m, k, d, c=None):
        c = core if c is None else c
        if k == 0:
            return wbuf.at[m, c, 0, (z + d + 4) % 4]
        return wbuf.at[m, c, 1, :, (y + d + 4) % 4]

    def plane_half(m, k, d, which):
        part = pl.ds(2 * which, 2)
        if k == 0:
            return wbuf.at[m, core, 0, (z + d + 4) % 4, part]
        return wbuf.at[m, core, 1, part, (y + d + 4) % 4]

    pairs = [(k, j) for k in range(2) for j in range(2)]

    def c_local(m):
        return pltpu.make_async_copy(w_in.at[m], wbuf.at[m, core, xl, z, y], loc_w.at[m])

    def c0(m):
        return remote(w_in.at[m], wbuf.at[m, core, xl, z, y], s0.at[m], r0.at[m], across)

    def c1(m, k, j):
        return remote(shard(m, k, 0), shard(m, k, 0), s1.at[m, k, j], r1.at[m, k, j], first_axis[k](steps[j]))

    def c1f(m, k, j):
        ref = shard(m, k, -steps[j]).at[pl.ds(32 * j, 32)]
        return remote(ref, ref, s1f.at[m, k, j], r1f.at[m, k, j], first_axis[k](steps[j]))

    def c2(m, k, j):
        return remote(plane(m, k, 0), plane(m, k, 0), s2.at[m, k, j], r2.at[m, k, j], second_axis[k](steps[j]))

    def c2f(m, k, j):
        ref = plane_half(m, k, -steps[j], j)
        return remote(ref, ref, s2f.at[m, k, j], r2f.at[m, k, j], second_axis[k](steps[j]))

    def c3(m, k, p):
        ref = plane(m, k, (0, -1, 1, 2)[p])
        return remote(ref, ref, s3.at[m, k, p], r3.at[m, k, p], sibling)

    def row_start(m):
        c_local(m).wait()
        c0(m).wait_recv()
        for k, j in pairs:
            c1(m, k, j).start()

    def row_pass(m):
        for k, j in pairs:
            c1(m, k, j).wait_recv()
            c1f(m, k, j).start()

    def row_end(m):
        for k, j in pairs:
            c1f(m, k, j).wait_recv()

    def row_gather(m):
        row_start(m)
        row_pass(m)
        row_end(m)

    def plane_start(m):
        for k, j in pairs:
            c2(m, k, j).start()
        for k in range(2):
            c3(m, k, 0).start()

    def plane_pass(m):
        for k, j in pairs:
            c2(m, k, j).wait_recv()
            c2f(m, k, j).start()
            c3(m, k, 1 + j).start()

    def plane_end(m):
        for k, j in pairs:
            c2f(m, k, j).wait_recv()
        for k in range(2):
            c3(m, k, 3).start()

    def weights_ready(m):
        for k in range(2):
            for p in range(4):
                c3(m, k, p).wait_recv()

    def peer(j):
        return (me + j) % 4

    def rows_of(c):
        return (HALO, CH - HALO) if c == 0 else (CH * c, CH)

    def h_main(c, j):
        to = peer(j)
        start, size = rows_of(c)
        base = ((to + 2 * half) % 4) * PART + start - HALO
        return remote(
            stream.at[pl.ds(pl.multiple_of(base, 16), size)], hbuf.at[me, pl.ds(start, size)],
            sh.at[c, j], rh.at[c, me], (sp, 4 * half + to),
        )

    def h_main_wait(c, j):
        start, size = rows_of(c)
        ref = hbuf.at[peer(j), pl.ds(start, size)]
        return remote(ref, ref, sh.at[c, j], rh.at[c, peer(j)], (sp, 4 * half + peer(j)))

    def h_main_local(c):
        start, size = rows_of(c)
        base = mine * PART + start - HALO
        return pltpu.make_async_copy(
            stream.at[pl.ds(pl.multiple_of(base, 16), size)], hbuf.at[me, pl.ds(start, size)], loc_h.at[c]
        )

    def h_halo(j):
        to = peer(j)
        quarter = (to + 2 * half) % 4
        base = (quarter * PART + TOK - HALO) % TOK
        to_sp = (sp + 1 - (quarter + 3) // 4) % 16
        return remote(
            stream.at[pl.ds(pl.multiple_of(base, 16), HALO)], hbuf.at[me, pl.ds(0, HALO)],
            shh.at[j], rhh.at[me], (to_sp, 4 * half + to),
        )

    def h_halo_wait(j):
        ref = hbuf.at[peer(j), pl.ds(0, HALO)]
        return remote(ref, ref, shh.at[j], rhh.at[peer(j)], (sp, 4 * half + peer(3)))

    def h_halo_local():
        base = (mine * PART + TOK - HALO) % TOK
        return pltpu.make_async_copy(
            stream.at[pl.ds(pl.multiple_of(base, 16), HALO)], hbuf.at[me, pl.ds(0, HALO)], loc_hh.at[0]
        )

    def labels():
        return remote(docs.at[pl.ds(15, 1)], ext.at[pl.ds(7, 1)], sl.at[0], rl.at[0], ((sp + 1) % 16, tp))

    for m in range(MATS):
        c_local(m).start()
    c0(0).start()
    labels().start()
    for j in range(1, 4):
        h_halo(j).start()

    @pl.when(mine == 0)
    def _():
        h_halo(0).start()

    @pl.when(mine != 0)
    def _():
        h_halo_local().start()

    for c in range(CHUNKS):
        h_main_local(c).start()
        for j in range(1, 4):
            h_main(c, j).start()
        if c == 0:
            c0(1).start()
    for m in range(2, MATS):
        c0(m).start()

    row_start(0)

    zbuf[...] = jnp.zeros_like(zbuf)
    sqbuf[...] = jnp.zeros_like(sqbuf)
    ext[8:24, :] = docs[...]
    labels().wait_recv()
    label_rows = []
    for k in range(5):
        row = (ext[pl.ds(4 * mine + 7 + k, 1), :] + 1).astype(F32)
        if k == 0:
            row = jnp.where(jnp.logical_and(sp == 0, mine == 0), jnp.zeros_like(row), row)
        label_rows.append(row)
    t_id = lax.broadcasted_iota(jnp.int32, (128, 128), 0)
    s_id = lax.broadcasted_iota(jnp.int32, (128, 128), 1)
    back = t_id - s_id
    lane = lax.broadcasted_iota(jnp.int32, (1, 128), 1)
    for c in range(CHUNKS):
        first, off = divmod(128 - HALO - LEAD + CH * c, 128)
        if off == 0:
            window = label_rows[first]
        else:
            window = jnp.where(
                lane < 128 - off,
                pltpu.roll(label_rows[first], 128 - off, 1),
                pltpu.roll(label_rows[first + 1], 128 - off, 1),
            )
        across_lanes = jnp.broadcast_to(window, (128, 128))
        same = jnp.logical_and(across_lanes == across_lanes.T, back >= 0)
        for i, w in enumerate(WINDOWS):
            member = jnp.where(jnp.logical_and(same, back < w), 1.0, 0.0).astype(F32)
            count = jnp.sum(member, axis=1, keepdims=True)
            band[c, i] = member[LEAD:].astype(BF16)
            inv[c, i] = jnp.broadcast_to(1.0 / count, (128, 128))[LEAD:]

    row_pass(0)
    row_end(0)
    plane_start(0)
    row_gather(1)
    plane_pass(0)
    plane_start(1)
    plane_end(0)
    weights_ready(0)

    def rows_at(c):
        return pl.ds(pl.multiple_of(c * CH, 16), CH)

    def squares_of(wide):
        total = None
        for k in range(COLS // 128):
            piece = wide[:, k * 128 : (k + 1) * 128]
            total = piece * piece if total is None else total + piece * piece
        return total

    def gain_of(l, b):
        at = pl.ds(pl.multiple_of(half * WIDE + b * COLS, COLS), COLS)
        return norm_gain[l : l + 1, at].astype(F32)

    def send_x(s):
        return remote(own.at[s], got.at[s], sx.at[s], rx.at[s], partner)

    def send_sq(s):
        return remote(ssown.at[s], ssgot.at[s], sq.at[s], rq.at[s], partner)

    def project(l, s, squares):
        sqbuf[0:CH, :] = squares
        ssown[s] = jnp.broadcast_to(jnp.sum(sqbuf[...].T, axis=0, keepdims=True), (8, 128))
        send_sq(s).start()
        for n in range(4):
            rhs = jnp.concatenate(
                [wbuf[2 * l, b % 2, b // 2, n].reshape(256, COLS) for b in range(4)], axis=1
            )
            part = lax.dot_general(
                gbuf[...], rhs, (((1,), (1,)), ((), ())), preferred_element_type=F32
            )
            own[s, :, n * 256 : (n + 1) * 256] = part.astype(BF16)
        send_x(s).start()

    def mix(l, c, s):
        send_sq(s).wait_recv()
        send_x(s).wait_recv()
        scale = lax.rsqrt((ssown[s] + ssgot[s]) / D + EPS)[0:1]
        scale = jnp.broadcast_to(scale, (128, 128)).T[0:CH]
        zbuf[0:LEAD, :] = zbuf[CH : CH + LEAD, :]
        for i in range(GROUPS):
            at = slice(i * GROUP, (i + 1) * GROUP)
            summed = own[s, :, at].astype(F32) + got[s, :, at].astype(F32)
            zbuf[LEAD:, at] = (summed * scale).astype(BF16)
        for i in range(GROUPS):
            at = slice(i * GROUP, (i + 1) * GROUP)
            values = zbuf[:, at]
            total = jnp.dot(band[c, i % 4], values, preferred_element_type=F32)
            pooled = (total * inv[c, i % 4] - zbuf[LEAD:, at].astype(F32)).astype(BF16)
            blended = jnp.dot(pooled, mix_pool[l, i], preferred_element_type=F32)
            mbuf[:, at] = (blended * pool_gain[l : l + 1, at].astype(F32)).astype(BF16)

    def update(l, c, last):
        rows = rows_at(c)
        squares = None
        for b in range(4):
            weights = wbuf[2 * l + 1, b % 2, b // 2].reshape(POOL, COLS)
            change = jnp.dot(mbuf[...], weights, preferred_element_type=F32)
            new = (hbuf[b, rows, :].astype(F32) + change).astype(BF16)
            hbuf[b, rows, :] = new
            if not last:
                wide = new.astype(F32)
                squares = squares_of(wide) if squares is None else squares + squares_of(wide)
                gbuf[:, b * COLS : (b + 1) * COLS] = (wide * gain_of(l + 1, b)).astype(BF16)
        return squares

    def wait_rows(c):
        h_main_local(c).wait()
        for j in range(1, 4):
            h_main_wait(c, j).wait_recv()

    @pl.when(mine == 0)
    def _():
        h_halo_wait(0).wait_recv()

    @pl.when(mine != 0)
    def _():
        h_halo_local().wait()

    for j in range(1, 4):
        h_halo_wait(j).wait_recv()

    def enter(c, carry):
        for k in range(CHUNKS):

            @pl.when(c == k)
            def _(k=k):
                wait_rows(k)

        rows = rows_at(c)
        squares = None
        for b in range(4):
            wide = hbuf[b, rows, :].astype(F32)
            squares = squares_of(wide) if squares is None else squares + squares_of(wide)
            gbuf[:, b * COLS : (b + 1) * COLS] = (wide * gain_of(0, b)).astype(BF16)
        project(0, c, squares)
        return carry

    lax.fori_loop(0, CHUNKS, enter, 0)

    def advance(m, prepare):
        if m + 1 < MATS and prepare:
            row_gather(m + 1)
        plane_pass(m)
        if m + 1 < MATS:
            plane_start(m + 1)
        plane_end(m)
        weights_ready(m)

    def out_rows(c):
        start, size = rows_of(c)
        return start, size, mine * PART + start - HALO

    def send_out(c, j):
        start, size, base = out_rows(c)
        to = peer(j)
        return remote(
            hbuf.at[to, pl.ds(start, size)], out.at[pl.ds(pl.multiple_of(base, 16), size)],
            so.at[c, j], ro.at[c, me], (sp, 4 * half + to),
        )

    def keep_out(c):
        start, size, base = out_rows(c)
        return pltpu.make_async_copy(
            hbuf.at[me, pl.ds(start, size)], out.at[pl.ds(pl.multiple_of(base, 16), size)], loc_o.at[c]
        )

    def wait_out(c, j):
        start, size, _ = out_rows(c)
        frm = peer(j)
        base = ((frm + 2 * half) % 4) * PART + start - HALO
        ref = out.at[pl.ds(pl.multiple_of(base, 16), size)]
        return remote(ref, ref, so.at[c, j], ro.at[c, frm], (sp, 4 * half + frm))

    for l in range(LAYERS):
        last = l == LAYERS - 1
        advance(2 * l + 1, True)
        if not last:
            advance(2 * l + 2, True)

        def one(c, carry, l=l, last=last):
            s = l * CHUNKS + c
            mix(l, c, s)
            squares = update(l, c, last)
            if not last:
                project(l + 1, s + CHUNKS, squares)
            else:
                for k in range(CHUNKS):

                    @pl.when(c == k)
                    def _(k=k):
                        for j in range(1, 4):
                            send_out(k, j).start()
                        keep_out(k).start()

            return carry

        lax.fori_loop(0, CHUNKS, one, 0)

    for m in range(MATS):
        c0(m).wait_send()
        for k, j in pairs:
            c1(m, k, j).wait_send()
            c1f(m, k, j).wait_send()
            c2(m, k, j).wait_send()
            c2f(m, k, j).wait_send()
        for k in range(2):
            for p in range(4):
                c3(m, k, p).wait_send()
    labels().wait_send()
    for j in range(1, 4):
        h_halo(j).wait_send()

    @pl.when(mine == 0)
    def _():
        h_halo(0).wait_send()

    for c in range(CHUNKS):
        for j in range(1, 4):
            h_main(c, j).wait_send()
    for s in range(LAYERS * CHUNKS):
        send_x(s).wait_send()
        send_sq(s).wait_send()
    for c in range(CHUNKS):
        keep_out(c).wait()
        for j in range(1, 4):
            send_out(c, j).wait_send()
            wait_out(c, j).wait_recv()


def body(stream, doc_ids, norm_gain, proj_in, mix_pool, pool_gain, proj_out):
    weights = jnp.stack([jnp.swapaxes(proj_in, 1, 2), proj_out], axis=1)
    weights = weights.reshape(MATS, 64, COLS)
    dma = pltpu.SemaphoreType.DMA
    steps = LAYERS * CHUNKS
    vmem = pl.BlockSpec(memory_space=pltpu.VMEM)
    hbm = pl.BlockSpec(memory_space=pl.ANY)
    return pl.pallas_call(
        kernel,
        out_shape=jax.ShapeDtypeStruct((TOK, COLS), BF16),
        in_specs=[hbm, vmem, vmem, hbm, vmem, vmem],
        out_specs=hbm,
        scratch_shapes=[
            pltpu.VMEM((MATS, 2, 2, 4, 4, 64, COLS), BF16),
            pltpu.VMEM((4, HALO + PART, COLS), BF16),
            pltpu.VMEM((steps, CH, POOL), BF16),
            pltpu.VMEM((steps, CH, POOL), BF16),
            pltpu.VMEM((steps, 8, 128), F32),
            pltpu.VMEM((steps, 8, 128), F32),
            pltpu.VMEM((CH, WIDE), BF16),
            pltpu.VMEM((LEAD + CH, POOL), BF16),
            pltpu.VMEM((CH, POOL), BF16),
            pltpu.VMEM((128, 128), F32),
            pltpu.VMEM((CHUNKS, 4, CH, 128), BF16),
            pltpu.VMEM((CHUNKS, 4, CH, 128), F32),
            pltpu.VMEM((24, 128), jnp.int32),
            dma((MATS,)), dma((CHUNKS,)), dma((1,)), dma((CHUNKS,)),
            dma((MATS,)), dma((MATS,)),
            dma((MATS, 2, 2)), dma((MATS, 2, 2)), dma((MATS, 2, 2)), dma((MATS, 2, 2)),
            dma((MATS, 2, 2)), dma((MATS, 2, 2)), dma((MATS, 2, 2)), dma((MATS, 2, 2)),
            dma((MATS, 2, 4)), dma((MATS, 2, 4)),
            dma((CHUNKS, 4)), dma((CHUNKS, 4)), dma((4,)), dma((4,)), dma((1,)), dma((1,)),
            dma((steps,)), dma((steps,)), dma((steps,)), dma((steps,)),
            dma((CHUNKS, 4)), dma((CHUNKS, 4)),
        ],
        compiler_params=pltpu.CompilerParams(
            has_side_effects=True, vmem_limit_bytes=56 * 1024 * 1024
        ),
        name="mixers",
    )(stream, doc_ids.reshape(16, 128), norm_gain, weights, mix_pool, pool_gain)


def solution(mesh):
    in_specs = (P("sp", "tp"), P("sp"), P(), P(None, "tp", "sp"), P(), P(), P(None, "sp", "tp"))
    out_specs = P("sp", "tp")
    return jax.shard_map(body, mesh=mesh, in_specs=in_specs, out_specs=out_specs, check_vma=False)
```

```python
import jax
import jax.numpy as jnp
from jax import lax
from jax.experimental import pallas as pl
from jax.experimental.pallas import tpu as pltpu
from jax.sharding import PartitionSpec as P

MESH = pl.DeviceIdType.MESH
F32 = jnp.float32
BF16 = jnp.bfloat16

D = 4096
POOL = 1024
GROUP = 128
GROUPS = POOL // GROUP
LAYERS = 3
MATS = 2 * LAYERS
TOK = 2048
COLS = 512
PART = TOK // 4
WIDE = 4 * COLS
HALO = 48
LEAD = 16
CHUNKS = 5
CH = (HALO + PART) // CHUNKS
WINDOWS = (2, 4, 8, 16)
EPS = 1e-06


def kernel(
    stream, docs, norm_gain, w_in, w_out, mix_pool, pool_gain, out,
    wbuf, hbuf, own, got, ssown, ssgot, gbuf, zbuf, mbuf, sqbuf, band, inv, ext,
    loc_w, loc_h, loc_hh, loc_o,
    s0, r0, s1, r1, s1f, r1f, s2, r2, s2f, r2f, s3, r3,
    sh, rh, shh, rhh, sl, rl, sx, rx, sq, rq, so, ro,
):
    sp = lax.axis_index("sp")
    tp = lax.axis_index("tp")
    z, y = sp // 4, sp % 4
    x, core = tp // 2, tp % 2
    half, xl = x // 2, x % 2
    me = xl * 2 + core
    mine = (me + 2 * half) % 4

    def remote(src, dst, send, recv, device):
        return pltpu.make_async_remote_copy(
            src_ref=src, dst_ref=dst, send_sem=send, recv_sem=recv,
            device_id=device, device_id_type=MESH,
        )

    across = (sp, (2 * half + 1 - xl) * 2 + core)
    partner = (sp, (3 - x) * 2 + core)
    sibling = (sp, x * 2 + 1 - core)

    def along_y(d):
        return (z * 4 + (y + d + 4) % 4, tp)

    def along_z(d):
        return (((z + d + 4) % 4) * 4 + y, tp)

    first_axis = (along_y, along_z)
    second_axis = (along_z, along_y)
    steps = (1, -1)

    def shard(m, k, d):
        if k == 0:
            return wbuf.at[m, core, 0, z, (y + d + 4) % 4]
        return wbuf.at[m, core, 1, (z + d + 4) % 4, y]

    def plane(m, k, d, c=None):
        c = core if c is None else c
        if k == 0:
            return wbuf.at[m, c, 0, (z + d + 4) % 4]
        return wbuf.at[m, c, 1, :, (y + d + 4) % 4]

    def plane_half(m, k, d, which):
        part = pl.ds(2 * which, 2)
        if k == 0:
            return wbuf.at[m, core, 0, (z + d + 4) % 4, part]
        return wbuf.at[m, core, 1, part, (y + d + 4) % 4]

    pairs = [(k, j) for k in range(2) for j in range(2)]

    def c_local(m):
        source = w_in if m % 2 == 0 else w_out
        return pltpu.make_async_copy(source.at[m // 2], wbuf.at[m, core, xl, z, y], loc_w.at[m])

    def c0(m):
        return remote(wbuf.at[m, core, xl, z, y], wbuf.at[m, core, xl, z, y], s0.at[m], r0.at[m], across)

    def c1(m, k, j):
        return remote(shard(m, k, 0), shard(m, k, 0), s1.at[m, k, j], r1.at[m, k, j], first_axis[k](steps[j]))

    def c1f(m, k, j):
        ref = shard(m, k, -steps[j]).at[pl.ds(32 * j, 32)]
        return remote(ref, ref, s1f.at[m, k, j], r1f.at[m, k, j], first_axis[k](steps[j]))

    def c2(m, k, j, p):
        ref = shard(m, k, (0, -1, 1, 2)[p])
        return remote(ref, ref, s2.at[m, k, j, p], r2.at[m, k, j, p], second_axis[k](steps[j]))

    def c2f(m, k, j):
        ref = plane_half(m, k, -steps[j], j)
        return remote(ref, ref, s2f.at[m, k, j], r2f.at[m, k, j], second_axis[k](steps[j]))

    def c3(m, k, p):
        ref = plane(m, k, (0, -1, 1, 2)[p])
        return remote(ref, ref, s3.at[m, k, p], r3.at[m, k, p], sibling)

    def row_start(m):
        c0(m).wait_recv()
        for k, j in pairs:
            c1(m, k, j).start()
        for k, j in pairs:
            c2(m, k, j, 0).start()

    def row_pass(m):
        for k, j in pairs:
            c1(m, k, j).wait_recv()
            c1f(m, k, j).start()
        for k, j in pairs:
            c2(m, k, 0, 1 + j).start()
            c2(m, k, 1, 1 + j).start()

    def row_end(m):
        for k in range(2):
            for j in range(2):
                c1f(m, k, j).wait_recv()
            c2(m, k, 0, 3).start()
            c2(m, k, 1, 3).start()
            c3(m, k, 0).start()

    def plane_pass(m):
        for k, j in pairs:
            for p in range(4):
                c2(m, k, j, p).wait_recv()
            c2f(m, k, j).start()
            c3(m, k, 1 + j).start()

    def plane_end(m):
        for k, j in pairs:
            c2f(m, k, j).wait_recv()
        for k in range(2):
            c3(m, k, 3).start()

    def weights_ready(m):
        for k in range(2):
            for p in range(4):
                c3(m, k, p).wait_recv()

    def peer(j):
        return (me + j) % 4

    def rows_of(c):
        return (HALO, CH - HALO) if c == 0 else (CH * c, CH)

    def h_main(c, j):
        to = peer(j)
        start, size = rows_of(c)
        base = ((to + 2 * half) % 4) * PART + start - HALO
        return remote(
            stream.at[pl.ds(pl.multiple_of(base, 16), size)], hbuf.at[me, pl.ds(start, size)],
            sh.at[c, j], rh.at[c, me], (sp, 4 * half + to),
        )

    def h_main_wait(c, j):
        start, size = rows_of(c)
        ref = hbuf.at[peer(j), pl.ds(start, size)]
        return remote(ref, ref, sh.at[c, j], rh.at[c, peer(j)], (sp, 4 * half + peer(j)))

    def h_main_local(c):
        start, size = rows_of(c)
        base = mine * PART + start - HALO
        return pltpu.make_async_copy(
            stream.at[pl.ds(pl.multiple_of(base, 16), size)], hbuf.at[me, pl.ds(start, size)], loc_h.at[c]
        )

    def h_halo(j):
        to = peer(j)
        quarter = (to + 2 * half) % 4
        base = (quarter * PART + TOK - HALO) % TOK
        to_sp = (sp + 1 - (quarter + 3) // 4) % 16
        return remote(
            stream.at[pl.ds(pl.multiple_of(base, 16), HALO)], hbuf.at[me, pl.ds(0, HALO)],
            shh.at[j], rhh.at[me], (to_sp, 4 * half + to),
        )

    def h_halo_wait(j):
        ref = hbuf.at[peer(j), pl.ds(0, HALO)]
        return remote(ref, ref, shh.at[j], rhh.at[peer(j)], (sp, 4 * half + peer(3)))

    def h_halo_local():
        base = (mine * PART + TOK - HALO) % TOK
        return pltpu.make_async_copy(
            stream.at[pl.ds(pl.multiple_of(base, 16), HALO)], hbuf.at[me, pl.ds(0, HALO)], loc_hh.at[0]
        )

    def labels():
        return remote(docs.at[pl.ds(15, 1)], ext.at[pl.ds(7, 1)], sl.at[0], rl.at[0], ((sp + 1) % 16, tp))

    for m in range(MATS):
        c_local(m).start()
    greeted = [across, partner, sibling, (sp, (2 * half + 1 - xl) * 2 + 1 - core)]
    greeted += [along_y(1), along_y(-1), along_z(1), along_z(-1)]
    for j in range(4):
        greeted += [((sp + 1) % 16, 4 * half + peer(j)), ((sp + 15) % 16, 4 * half + peer(j))]
    barrier = pltpu.get_barrier_semaphore()
    for device in greeted:
        pl.semaphore_signal(barrier, inc=1, device_id=device, device_id_type=MESH)
    pl.semaphore_wait(barrier, len(greeted))

    for m in range(3):
        c_local(m).wait()
        c0(m).start()
    labels().start()
    for j in range(1, 4):
        h_halo(j).start()

    @pl.when(mine == 0)
    def _():
        h_halo(0).start()

    @pl.when(mine != 0)
    def _():
        h_halo_local().start()

    for c in range(CHUNKS):
        h_main_local(c).start()
        for j in range(1, 4):
            h_main(c, j).start()
        if c == 2:
            c_local(3).wait()
            c0(3).start()
    for m in range(4, MATS):
        c_local(m).wait()
        c0(m).start()

    row_start(0)

    zbuf[...] = jnp.zeros_like(zbuf)
    sqbuf[...] = jnp.zeros_like(sqbuf)
    for l in range(1, LAYERS):
        got[l * CHUNKS, 0 : LEAD * l, :] = jnp.zeros((LEAD * l, POOL), BF16)
    ext[8:24, :] = docs[...]
    labels().wait_recv()
    label_rows = []
    for k in range(5):
        row = (ext[pl.ds(4 * mine + 7 + k, 1), :] + 1).astype(F32)
        if k == 0:
            row = jnp.where(jnp.logical_and(sp == 0, mine == 0), jnp.zeros_like(row), row)
        label_rows.append(row)
    t_id = lax.broadcasted_iota(jnp.int32, (128, 128), 0)
    s_id = lax.broadcasted_iota(jnp.int32, (128, 128), 1)
    back = t_id - s_id
    lane = lax.broadcasted_iota(jnp.int32, (1, 128), 1)
    for c in range(CHUNKS):
        first, off = divmod(128 - HALO - LEAD + CH * c, 128)
        if off == 0:
            window = label_rows[first]
        else:
            window = jnp.where(
                lane < 128 - off,
                pltpu.roll(label_rows[first], 128 - off, 1),
                pltpu.roll(label_rows[first + 1], 128 - off, 1),
            )
        across_lanes = jnp.broadcast_to(window, (128, 128))
        same = jnp.logical_and(across_lanes == across_lanes.T, back >= 0)
        for i, w in enumerate(WINDOWS):
            member = jnp.where(jnp.logical_and(same, back < w), 1.0, 0.0).astype(F32)
            count = jnp.sum(member, axis=1, keepdims=True)
            band[c, i] = member[LEAD:].astype(BF16)
            inv[c, i] = jnp.broadcast_to(1.0 / count, (128, 128))[LEAD:]

    row_pass(0)
    row_end(0)
    row_start(1)
    plane_pass(0)
    row_pass(1)
    row_start(2)
    row_end(1)
    plane_end(0)
    weights_ready(0)

    def rows_at(c):
        return pl.ds(pl.multiple_of(c * CH, 16), CH)

    def squares_of(wide):
        total = None
        for k in range(COLS // 128):
            piece = wide[:, k * 128 : (k + 1) * 128]
            total = piece * piece if total is None else total + piece * piece
        return total

    def gain_of(l, b):
        at = pl.ds(pl.multiple_of(half * WIDE + b * COLS, COLS), COLS)
        return norm_gain[l : l + 1, at].astype(F32)

    def send_x(s, skip=0):
        rows = pl.ds(skip, CH - skip)
        return remote(own.at[s, rows], got.at[s, rows], sx.at[s], rx.at[s], partner)

    def on_x(l, c, s, act):
        if l == 0:
            act(send_x(s))
        else:

            @pl.when(c == 0)
            def _():
                act(send_x(s, LEAD * l))

            @pl.when(c != 0)
            def _():
                act(send_x(s))

    def send_sq(s):
        return remote(ssown.at[s], ssgot.at[s], sq.at[s], rq.at[s], partner)

    def project(l, c, s, squares):
        sqbuf[0:CH, :] = squares
        ssown[s] = jnp.broadcast_to(jnp.sum(sqbuf[...].T, axis=0, keepdims=True), (8, 128))
        send_sq(s).start()
        for n in range(4):
            rhs = jnp.concatenate(
                [wbuf[2 * l, b % 2, b // 2, n].reshape(256, COLS) for b in range(4)], axis=1
            )
            part = lax.dot_general(
                gbuf[...], rhs, (((1,), (1,)), ((), ())), preferred_element_type=F32
            )
            own[s, :, n * 256 : (n + 1) * 256] = part.astype(BF16)
        on_x(l, c, s, lambda copy: copy.start())

    def mix(l, c, s):
        send_sq(s).wait_recv()
        on_x(l, c, s, lambda copy: copy.wait_recv())
        scale = lax.rsqrt((ssown[s] + ssgot[s]) / D + EPS)[0:1]
        scale = jnp.broadcast_to(scale, (128, 128)).T[0:CH]
        zbuf[0:LEAD, :] = zbuf[CH : CH + LEAD, :]
        for i in range(GROUPS):
            at = slice(i * GROUP, (i + 1) * GROUP)
            summed = own[s, :, at].astype(F32) + got[s, :, at].astype(F32)
            zbuf[LEAD:, at] = (summed * scale).astype(BF16)
        for i in range(GROUPS):
            at = slice(i * GROUP, (i + 1) * GROUP)
            values = zbuf[:, at]
            total = jnp.dot(band[c, i % 4], values, preferred_element_type=F32)
            pooled = (total * inv[c, i % 4] - zbuf[LEAD:, at].astype(F32)).astype(BF16)
            blended = jnp.dot(pooled, mix_pool[l, i], preferred_element_type=F32)
            mbuf[:, at] = (blended * pool_gain[l : l + 1, at].astype(F32)).astype(BF16)

    def update(l, c):
        rows = rows_at(c)
        squares = None
        for b in range(4):
            weights = wbuf[2 * l + 1, b % 2, b // 2].reshape(POOL, COLS)
            change = jnp.dot(mbuf[...], weights, preferred_element_type=F32)
            new = (hbuf[b, rows, :].astype(F32) + change).astype(BF16)
            hbuf[b, rows, :] = new
            wide = new.astype(F32)
            squares = squares_of(wide) if squares is None else squares + squares_of(wide)
            gbuf[:, b * COLS : (b + 1) * COLS] = (wide * gain_of(l + 1, b)).astype(BF16)
        return squares

    def finish(c):
        rows = rows_at(c)
        for j in (2, 3, 1, 0):
            b = peer(j)
            weights = wbuf[MATS - 1, b % 2, b // 2].reshape(POOL, COLS)
            change = jnp.dot(mbuf[...], weights, preferred_element_type=F32)
            hbuf[b, rows, :] = (hbuf[b, rows, :].astype(F32) + change).astype(BF16)
            for first in (True, False):

                @pl.when(c == 0 if first else c != 0)
                def _(j=j, first=first):
                    (send_out(c, j, first) if j else keep_out(c, first)).start()

    def wait_rows(c):
        h_main_local(c).wait()
        for j in range(1, 4):
            h_main_wait(c, j).wait_recv()

    @pl.when(mine == 0)
    def _():
        h_halo_wait(0).wait_recv()

    @pl.when(mine != 0)
    def _():
        h_halo_local().wait()

    for j in range(1, 4):
        h_halo_wait(j).wait_recv()

    def enter(c, carry):
        for k in range(CHUNKS):

            @pl.when(c == k)
            def _(k=k):
                wait_rows(k)

        rows = rows_at(c)
        squares = None
        for b in range(4):
            wide = hbuf[b, rows, :].astype(F32)
            squares = squares_of(wide) if squares is None else squares + squares_of(wide)
            gbuf[:, b * COLS : (b + 1) * COLS] = (wide * gain_of(0, b)).astype(BF16)
        project(0, c, c, squares)

        @pl.when(c == 2)
        def _():
            row_pass(2)

        return carry

    lax.fori_loop(0, CHUNKS, enter, 0)

    plane_pass(1)
    row_end(2)
    row_start(3)
    plane_end(1)
    weights_ready(1)
    plane_pass(2)
    row_pass(3)
    row_start(4)
    plane_end(2)
    row_end(3)
    weights_ready(2)

    def out_rows(c, quarter, first):
        start, size = (HALO, CH - HALO) if first else (c * CH, CH)
        base = pl.multiple_of(quarter * PART + start - HALO, 16)
        return pl.ds(start if first else pl.multiple_of(start, 16), size), pl.ds(base, size)

    def send_out(c, j, first):
        here, there = out_rows(c, mine, first)
        to = peer(j)
        return remote(
            hbuf.at[to, here], out.at[there], so.at[c, j], ro.at[c, me], (sp, 4 * half + to)
        )

    def keep_out(c, first):
        here, there = out_rows(c, mine, first)
        return pltpu.make_async_copy(hbuf.at[me, here], out.at[there], loc_o.at[c])

    def wait_out(c, j, first):
        frm = peer(j)
        _, there = out_rows(c, (frm + 2 * half) % 4, first)
        ref = out.at[there]
        return remote(ref, ref, so.at[c, j], ro.at[c, frm], (sp, 4 * half + frm))

    for l in range(LAYERS):
        last = l == LAYERS - 1
        if l == 1:
            row_end(4)
            plane_end(3)
            weights_ready(3)
            row_pass(5)
            plane_pass(4)
            row_end(5)
            plane_end(4)
            weights_ready(4)
        if l == 2:
            plane_end(5)
            weights_ready(5)

        def one(c, carry, l=l, last=last):
            s = l * CHUNKS + c
            mix(l, c, s)
            if last:
                finish(c)
            else:
                project(l + 1, c, s + CHUNKS, update(l, c))

                @pl.when(c == (2 if l == 0 else 0))
                def _():
                    if l == 0:
                        plane_pass(3)
                        row_pass(4)
                        row_start(5)
                    else:
                        plane_pass(5)

            return carry

        lax.fori_loop(0, CHUNKS, one, 0)

    for m in range(MATS):
        c0(m).wait_send()
        for k, j in pairs:
            c1(m, k, j).wait_send()
            c1f(m, k, j).wait_send()
            for p in range(4):
                c2(m, k, j, p).wait_send()
            c2f(m, k, j).wait_send()
        for k in range(2):
            for p in range(4):
                c3(m, k, p).wait_send()
    labels().wait_send()
    for j in range(1, 4):
        h_halo(j).wait_send()

    @pl.when(mine == 0)
    def _():
        h_halo(0).wait_send()

    for c in range(CHUNKS):
        for j in range(1, 4):
            h_main(c, j).wait_send()
    for s in range(LAYERS * CHUNKS):
        send_x(s, LEAD * (s // CHUNKS) if s % CHUNKS == 0 else 0).wait_send()
        send_sq(s).wait_send()
    for c in range(CHUNKS):
        keep_out(c, c == 0).wait()
        for j in range(1, 4):
            send_out(c, j, c == 0).wait_send()
            wait_out(c, j, c == 0).wait_recv()


def body(stream, doc_ids, norm_gain, proj_in, mix_pool, pool_gain, proj_out):
    dma = pltpu.SemaphoreType.DMA
    steps = LAYERS * CHUNKS
    vmem = pl.BlockSpec(memory_space=pltpu.VMEM)
    hbm = pl.BlockSpec(memory_space=pl.ANY)
    return pl.pallas_call(
        kernel,
        out_shape=pltpu.VMEM((TOK, COLS), BF16),
        in_specs=[hbm, vmem, vmem, hbm, hbm, vmem, vmem],
        out_specs=vmem,
        scratch_shapes=[
            pltpu.VMEM((MATS, 2, 2, 4, 4, 64, COLS), BF16),
            pltpu.VMEM((4, HALO + PART, COLS), BF16),
            pltpu.VMEM((steps, CH, POOL), BF16),
            pltpu.VMEM((steps, CH, POOL), BF16),
            pltpu.VMEM((steps, 8, 128), F32),
            pltpu.VMEM((steps, 8, 128), F32),
            pltpu.VMEM((CH, WIDE), BF16),
            pltpu.VMEM((LEAD + CH, POOL), BF16),
            pltpu.VMEM((CH, POOL), BF16),
            pltpu.VMEM((128, 128), F32),
            pltpu.VMEM((CHUNKS, 4, CH, 128), BF16),
            pltpu.VMEM((CHUNKS, 4, CH, 128), F32),
            pltpu.VMEM((24, 128), jnp.int32),
            dma((MATS,)), dma((CHUNKS,)), dma((1,)), dma((CHUNKS,)),
            dma((MATS,)), dma((MATS,)),
            dma((MATS, 2, 2)), dma((MATS, 2, 2)), dma((MATS, 2, 2)), dma((MATS, 2, 2)),
            dma((MATS, 2, 2, 4)), dma((MATS, 2, 2, 4)), dma((MATS, 2, 2)), dma((MATS, 2, 2)),
            dma((MATS, 2, 4)), dma((MATS, 2, 4)),
            dma((CHUNKS, 4)), dma((CHUNKS, 4)), dma((4,)), dma((4,)), dma((1,)), dma((1,)),
            dma((steps,)), dma((steps,)), dma((steps,)), dma((steps,)),
            dma((CHUNKS, 4)), dma((CHUNKS, 4)),
        ],
        compiler_params=pltpu.CompilerParams(
            has_side_effects=True, collective_id=0, vmem_limit_bytes=56 * 1024 * 1024
        ),
        name="mixers",
    )(
        stream, doc_ids.reshape(16, 128), norm_gain, jnp.swapaxes(proj_in, 1, 2), proj_out,
        mix_pool, pool_gain,
    )


def solution(mesh):
    in_specs = (P("sp", "tp"), P("sp"), P(), P(None, "tp", "sp"), P(), P(), P(None, "sp", "tp"))
    out_specs = P("sp", "tp")
    return jax.shard_map(body, mesh=mesh, in_specs=in_specs, out_specs=out_specs, check_vma=False)
```

```python
import jax
import jax.numpy as jnp
from jax import lax
from jax.experimental import pallas as pl
from jax.experimental.pallas import tpu as pltpu
from jax.sharding import PartitionSpec as P

MESH = pl.DeviceIdType.MESH
F32 = jnp.float32
BF16 = jnp.bfloat16

D = 4096
POOL = 1024
GROUP = 128
GROUPS = POOL // GROUP
LAYERS = 3
MATS = 2 * LAYERS
TOK = 2048
COLS = 512
PART = TOK // 4
WIDE = 4 * COLS
HALO = 48
LEAD = 16
CHUNKS = 5
CH = (HALO + PART) // CHUNKS
WINDOWS = (2, 4, 8, 16)
STEPS = LAYERS * CHUNKS
SPLIT = 64
EPS = 1e-06


def kernel(
    stream, docs, norm_gain, w_in, w_out, mix_hbm, pool_gain, out,
    wbuf, hbuf, own, got, ssown, ssgot, gbuf, zbuf, mbuf, sqbuf, band, inv, ext, mix_pool,
    loc_w, loc_h, loc_hh, loc_o, loc_m,
    s0, r0, s1, r1, s1f, r1f, s2, r2, s2f, r2f, s3, r3,
    sh, rh, shh, rhh, sl, rl, sx, rx, sq, rq, so, ro,
):
    sp = lax.axis_index("sp")
    tp = lax.axis_index("tp")
    z, y = sp // 4, sp % 4
    x, core = tp // 2, tp % 2
    half, xl = x // 2, x % 2
    me = xl * 2 + core
    mine = (me + 2 * half) % 4

    def remote(src, dst, send, recv, device):
        return pltpu.make_async_remote_copy(
            src_ref=src, dst_ref=dst, send_sem=send, recv_sem=recv,
            device_id=device, device_id_type=MESH,
        )

    across = (sp, (2 * half + 1 - xl) * 2 + core)
    partner = (sp, (3 - x) * 2 + core)
    sibling = (sp, x * 2 + 1 - core)

    def along_y(d):
        return (z * 4 + (y + d + 4) % 4, tp)

    def along_z(d):
        return (((z + d + 4) % 4) * 4 + y, tp)

    first_axis = (along_y, along_z)
    second_axis = (along_z, along_y)
    steps = (1, -1)

    def shard(m, k, d):
        if k == 0:
            return wbuf.at[m, core, 0, z, (y + d + 4) % 4]
        return wbuf.at[m, core, 1, (z + d + 4) % 4, y]

    def plane(m, k, d, c=None):
        c = core if c is None else c
        if k == 0:
            return wbuf.at[m, c, 0, (z + d + 4) % 4]
        return wbuf.at[m, c, 1, :, (y + d + 4) % 4]

    def plane_half(m, k, d, which):
        part = pl.ds(2 * which, 2)
        if k == 0:
            return wbuf.at[m, core, 0, (z + d + 4) % 4, part]
        return wbuf.at[m, core, 1, part, (y + d + 4) % 4]

    pairs = [(k, j) for k in range(2) for j in range(2)]

    def c_local(m):
        source = w_in if m % 2 == 0 else w_out
        return pltpu.make_async_copy(source.at[m // 2], wbuf.at[m, core, xl, z, y], loc_w.at[m])

    def c0(m):
        return remote(wbuf.at[m, core, xl, z, y], wbuf.at[m, core, xl, z, y], s0.at[m], r0.at[m], across)

    def c1(m, k, j):
        return remote(shard(m, k, 0), shard(m, k, 0), s1.at[m, k, j], r1.at[m, k, j], first_axis[k](steps[j]))

    def c1f(m, k, j):
        ref = shard(m, k, -steps[j]).at[pl.ds(32 * j, 32)]
        return remote(ref, ref, s1f.at[m, k, j], r1f.at[m, k, j], first_axis[k](steps[j]))

    def c2(m, k, j, p):
        ref = shard(m, k, (0, -1, 1, 2)[p]) if m == 0 else plane(m, k, 0)
        return remote(ref, ref, s2.at[m, k, j, p], r2.at[m, k, j, p], second_axis[k](steps[j]))

    def c2f(m, k, j):
        ref = plane_half(m, k, -steps[j], j)
        return remote(ref, ref, s2f.at[m, k, j], r2f.at[m, k, j], second_axis[k](steps[j]))

    def c3(m, k, p):
        ref = plane(m, k, (0, -1, 1, 2)[p])
        return remote(ref, ref, s3.at[m, k, p], r3.at[m, k, p], sibling)

    def parts_of(m):
        return range(4 if m == 0 else 1)

    def row_start(m):
        c0(m).wait_recv()
        for k, j in pairs:
            c1(m, k, j).start()
        if m == 0:
            for k, j in pairs:
                c2(m, k, j, 0).start()

    def row_pass(m):
        for k, j in pairs:
            c1(m, k, j).wait_recv()
            c1f(m, k, j).start()
        if m == 0:
            for k, j in pairs:
                c2(m, k, 0, 1 + j).start()
                c2(m, k, 1, 1 + j).start()

    def row_end(m):
        for k in range(2):
            for j in range(2):
                c1f(m, k, j).wait_recv()
            for j in range(2):
                c2(m, k, j, 3 if m == 0 else 0).start()
            c3(m, k, 0).start()

    def plane_pass(m):
        for k, j in pairs:
            for p in parts_of(m):
                c2(m, k, j, p).wait_recv()
            c2f(m, k, j).start()
            c3(m, k, 1 + j).start()

    def plane_end(m):
        for k, j in pairs:
            c2f(m, k, j).wait_recv()
        for k in range(2):
            c3(m, k, 3).start()

    def weights_ready(m):
        for k in range(2):
            for p in range(4):
                c3(m, k, p).wait_recv()

    def peer(j):
        return (me + j) % 4

    def rows_of(c):
        return (HALO, CH - HALO) if c == 0 else (CH * c, CH)

    def h_main(c, j):
        to = peer(j)
        start, size = rows_of(c)
        base = ((to + 2 * half) % 4) * PART + start - HALO
        return remote(
            stream.at[pl.ds(pl.multiple_of(base, 16), size)], hbuf.at[me, pl.ds(start, size)],
            sh.at[c, j], rh.at[c, me], (sp, 4 * half + to),
        )

    def h_main_wait(c, j):
        start, size = rows_of(c)
        ref = hbuf.at[peer(j), pl.ds(start, size)]
        return remote(ref, ref, sh.at[c, j], rh.at[c, peer(j)], (sp, 4 * half + peer(j)))

    def h_main_local(c):
        start, size = rows_of(c)
        base = mine * PART + start - HALO
        return pltpu.make_async_copy(
            stream.at[pl.ds(pl.multiple_of(base, 16), size)], hbuf.at[me, pl.ds(start, size)], loc_h.at[c]
        )

    def h_halo(j):
        to = peer(j)
        quarter = (to + 2 * half) % 4
        base = (quarter * PART + TOK - HALO) % TOK
        to_sp = (sp + 1 - (quarter + 3) // 4) % 16
        return remote(
            stream.at[pl.ds(pl.multiple_of(base, 16), HALO)], hbuf.at[me, pl.ds(0, HALO)],
            shh.at[j], rhh.at[me], (to_sp, 4 * half + to),
        )

    def h_halo_wait(j):
        ref = hbuf.at[peer(j), pl.ds(0, HALO)]
        return remote(ref, ref, shh.at[j], rhh.at[peer(j)], (sp, 4 * half + peer(3)))

    def h_halo_local():
        base = (mine * PART + TOK - HALO) % TOK
        return pltpu.make_async_copy(
            stream.at[pl.ds(pl.multiple_of(base, 16), HALO)], hbuf.at[me, pl.ds(0, HALO)], loc_hh.at[0]
        )

    def labels():
        return remote(docs.at[pl.ds(15, 1)], ext.at[pl.ds(7, 1)], sl.at[0], rl.at[0], ((sp + 1) % 16, tp))

    mix_copy = pltpu.make_async_copy(mix_hbm, mix_pool, loc_m.at[0])
    for m in range(MATS):
        c_local(m).start()
    mix_copy.start()
    greeted = [across, partner, sibling, (sp, (2 * half + 1 - xl) * 2 + 1 - core)]
    greeted += [along_y(1), along_y(-1), along_z(1), along_z(-1)]
    barrier = pltpu.get_barrier_semaphore()
    for device in greeted:
        pl.semaphore_signal(barrier, inc=1, device_id=device, device_id_type=MESH)

    @pl.when(mine == 0)
    def _():
        for j in range(4):
            device = ((sp + 15) % 16, 4 * half + peer(j))
            pl.semaphore_signal(barrier, inc=1, device_id=device, device_id_type=MESH)

    pl.semaphore_wait(barrier, len(greeted) + 1)

    for m in range(3):
        c_local(m).wait()
        c0(m).start()
    for j in range(1, 4):
        h_halo(j).start()

    @pl.when(mine == 0)
    def _():
        labels().start()
        h_halo(0).start()

    @pl.when(mine != 0)
    def _():
        h_halo_local().start()

    for c in range(CHUNKS):
        h_main_local(c).start()
        for j in range(1, 4):
            h_main(c, j).start()
        if c == 2:
            c_local(3).wait()
            c0(3).start()
    for m in range(4, MATS):
        c_local(m).wait()
        c0(m).start()

    row_start(0)

    zbuf[...] = jnp.zeros_like(zbuf)
    sqbuf[...] = jnp.zeros_like(sqbuf)
    for l in range(1, LAYERS):
        got[l * CHUNKS, 0 : LEAD * l, :] = jnp.zeros((LEAD * l, POOL), BF16)
    ext[8:24, :] = docs[...]

    @pl.when(mine == 0)
    def _():
        labels().wait_recv()

    label_rows = []
    for k in range(5):
        row = (ext[pl.ds(4 * mine + 7 + k, 1), :] + 1).astype(F32)
        if k == 0:
            row = jnp.where(jnp.logical_and(sp == 0, mine == 0), jnp.zeros_like(row), row)
        label_rows.append(row)
    t_id = lax.broadcasted_iota(jnp.int32, (128, 128), 0)
    s_id = lax.broadcasted_iota(jnp.int32, (128, 128), 1)
    back = t_id - s_id
    lane = lax.broadcasted_iota(jnp.int32, (1, 128), 1)
    for c in range(CHUNKS):
        first, off = divmod(128 - HALO - LEAD + CH * c, 128)
        if off == 0:
            window = label_rows[first]
        else:
            window = jnp.where(
                lane < 128 - off,
                pltpu.roll(label_rows[first], 128 - off, 1),
                pltpu.roll(label_rows[first + 1], 128 - off, 1),
            )
        across_lanes = jnp.broadcast_to(window, (128, 128))
        same = jnp.logical_and(across_lanes == across_lanes.T, back >= 0)
        for i, w in enumerate(WINDOWS):
            member = jnp.where(jnp.logical_and(same, back < w), 1.0, 0.0).astype(F32)
            count = jnp.sum(member, axis=1, keepdims=True)
            band[c, i] = member[LEAD:].astype(BF16)
            inv[c, i] = jnp.broadcast_to(1.0 / count, (128, 128))[LEAD:]

    row_pass(0)
    row_end(0)
    row_start(1)
    row_start(2)
    plane_pass(0)
    row_pass(1)
    row_pass(2)
    row_start(3)
    plane_end(0)
    row_end(1)
    weights_ready(0)
    row_end(2)

    def rows_at(c):
        return pl.ds(pl.multiple_of(c * CH, 16), CH)

    def squares_of(wide):
        total = None
        for k in range(COLS // 128):
            piece = wide[:, k * 128 : (k + 1) * 128]
            total = piece * piece if total is None else total + piece * piece
        return total

    def gain_of(l, b):
        at = pl.ds(pl.multiple_of(half * WIDE + b * COLS, COLS), COLS)
        return norm_gain[l : l + 1, at].astype(F32)

    def send_x(s, at, rows=(0, CH), lanes=(0, POOL)):
        index = (s, pl.ds(*rows), pl.ds(*lanes))
        return remote(own.at[index], got.at[index], sx.at[at], rx.at[at], partner)

    def x_first(n):
        return send_x(0, STEPS + 1 + n, lanes=(n * 256, 256))

    def x_kept(l, c, s):
        if c == 0 and l > 0:
            return [send_x(s, s, rows=(LEAD * l, CH - LEAD * l))]
        if c == CHUNKS - 1 and l == LAYERS - 1:
            return [send_x(s, s, rows=(0, SPLIT)), send_x(s, STEPS, rows=(SPLIT, CH - SPLIT))]
        if c == 0:
            return [x_first(n) for n in range(4)]
        return [send_x(s, s)]

    def on_x(l, c, s, act):
        special = [0, CHUNKS - 1] if l == LAYERS - 1 else [0]
        plain = c != 0
        for k in special:

            @pl.when(c == k)
            def _(k=k):
                for copy in x_kept(l, k, s):
                    act(copy)

            plain = jnp.logical_and(plain, c != k)

        @pl.when(plain)
        def _():
            act(send_x(s, s))

    def send_sq(s):
        return remote(ssown.at[s], ssgot.at[s], sq.at[s], rq.at[s], partner)

    def project(l, c, s, squares):
        sqbuf[0:CH, :] = squares
        ssown[s] = jnp.broadcast_to(jnp.sum(sqbuf[...].T, axis=0, keepdims=True), (8, 128))
        send_sq(s).start()
        for n in range(4):
            rhs = jnp.concatenate(
                [wbuf[2 * l, b % 2, b // 2, n].reshape(256, COLS) for b in range(4)], axis=1
            )
            part = lax.dot_general(
                gbuf[...], rhs, (((1,), (1,)), ((), ())), preferred_element_type=F32
            )
            own[s, :, n * 256 : (n + 1) * 256] = part.astype(BF16)
            if l == 0:

                @pl.when(c == 0)
                def _(n=n):
                    x_first(n).start()

        if l == 0:

            @pl.when(c != 0)
            def _():
                send_x(s, s).start()

        else:
            on_x(l, c, s, lambda copy: copy.start())

    def mix(l, c, s, first=0, size=CH):
        rows = slice(first, first + size)
        here = slice(LEAD + first, LEAD + first + size)
        if first == 0:
            send_sq(s).wait_recv()
            zbuf[0:LEAD, :] = zbuf[CH : CH + LEAD, :]
        scale = lax.rsqrt((ssown[s] + ssgot[s]) / D + EPS)[0:1]
        scale = jnp.broadcast_to(scale, (128, 128)).T[rows]
        for i in range(GROUPS):
            at = slice(i * GROUP, (i + 1) * GROUP)
            summed = own[s, rows, at].astype(F32) + got[s, rows, at].astype(F32)
            zbuf[here, at] = (summed * scale).astype(BF16)
        for i in range(GROUPS):
            at = slice(i * GROUP, (i + 1) * GROUP)
            total = jnp.dot(band[c, i % 4, rows], zbuf[:, at], preferred_element_type=F32)
            pooled = (total * inv[c, i % 4, rows] - zbuf[here, at].astype(F32)).astype(BF16)
            blended = jnp.dot(pooled, mix_pool[l, i], preferred_element_type=F32)
            mbuf[rows, at] = (blended * pool_gain[l : l + 1, at].astype(F32)).astype(BF16)

    def update(l, c):
        rows = rows_at(c)
        squares = None
        for b in range(4):
            weights = wbuf[2 * l + 1, b % 2, b // 2].reshape(POOL, COLS)
            change = jnp.dot(mbuf[...], weights, preferred_element_type=F32)
            new = (hbuf[b, rows, :].astype(F32) + change).astype(BF16)
            hbuf[b, rows, :] = new
            wide = new.astype(F32)
            squares = squares_of(wide) if squares is None else squares + squares_of(wide)
            gbuf[:, b * COLS : (b + 1) * COLS] = (wide * gain_of(l + 1, b)).astype(BF16)
        return squares

    def finish(c, first=0, size=CH):
        for j in (2, 3, 1, 0):
            b = peer(j)
            weights = wbuf[MATS - 1, b % 2, b // 2].reshape(POOL, COLS)
            change = jnp.dot(mbuf[first : first + size], weights, preferred_element_type=F32)
            rows = pl.ds(pl.multiple_of(c * CH + first, 16), size)
            hbuf[b, rows, :] = (hbuf[b, rows, :].astype(F32) + change).astype(BF16)
            if isinstance(c, int):
                at = c + (first > 0)
                (send_out(at, j, c * CH + first, size) if j else keep_out(at, c * CH + first, size)).start()
                continue
            for start, size_ in ((HALO, CH - HALO), (pl.multiple_of(c * CH, 16), CH)):

                @pl.when(c == 0 if size_ < CH else c != 0)
                def _(j=j, start=start, size_=size_):
                    (send_out(c, j, start, size_) if j else keep_out(c, start, size_)).start()

    def wait_rows(c):
        h_main_local(c).wait()
        for j in range(1, 4):
            h_main_wait(c, j).wait_recv()

    @pl.when(mine == 0)
    def _():
        h_halo_wait(0).wait_recv()

    @pl.when(mine != 0)
    def _():
        h_halo_local().wait()

    for j in range(1, 4):
        h_halo_wait(j).wait_recv()

    def enter(c, carry):
        for k in range(CHUNKS):

            @pl.when(c == k)
            def _(k=k):
                wait_rows(k)

        rows = rows_at(c)
        squares = None
        for b in range(4):
            wide = hbuf[b, rows, :].astype(F32)
            squares = squares_of(wide) if squares is None else squares + squares_of(wide)
            gbuf[:, b * COLS : (b + 1) * COLS] = (wide * gain_of(0, b)).astype(BF16)
        project(0, c, c, squares)

        @pl.when(c == 2)
        def _():
            row_pass(3)

        return carry

    lax.fori_loop(0, CHUNKS, enter, 0)

    plane_pass(1)
    row_start(4)
    plane_pass(2)
    row_end(3)
    plane_end(1)
    weights_ready(1)
    row_pass(4)
    row_start(5)
    plane_end(2)
    weights_ready(2)

    def out_rows(quarter, start, size):
        base = pl.multiple_of(quarter * PART + start - HALO, 16)
        return pl.ds(start, size), pl.ds(base, size)

    def send_out(at, j, start, size):
        here, there = out_rows(mine, start, size)
        to = peer(j)
        return remote(
            hbuf.at[to, here], out.at[there], so.at[at, j], ro.at[at, me], (sp, 4 * half + to)
        )

    def keep_out(at, start, size):
        here, there = out_rows(mine, start, size)
        return pltpu.make_async_copy(hbuf.at[me, here], out.at[there], loc_o.at[at])

    def wait_out(at, j, start, size):
        frm = peer(j)
        _, there = out_rows((frm + 2 * half) % 4, start, size)
        ref = out.at[there]
        return remote(ref, ref, so.at[at, j], ro.at[at, frm], (sp, 4 * half + frm))

    mix_copy.wait()
    for l in range(LAYERS):
        last = l == LAYERS - 1
        if l == 1:
            plane_end(3)
            weights_ready(3)
            plane_pass(4)
            row_end(5)
            plane_end(4)
            weights_ready(4)
        if l == 2:
            plane_end(5)
            weights_ready(5)

        def one(c, carry, l=l, last=last):
            s = l * CHUNKS + c
            on_x(l, c, s, lambda copy: copy.wait_recv())
            mix(l, c, s)
            if last:
                finish(c)
            else:
                project(l + 1, c, s + CHUNKS, update(l, c))

                @pl.when(c == 1)
                def _():
                    plane_pass(3 if l == 0 else 5)

                if l == 0:

                    @pl.when(c == 2)
                    def _():
                        row_end(4)
                        row_pass(5)

            return carry

        lax.fori_loop(0, CHUNKS - 1 if last else CHUNKS, one, 0)

    end = CHUNKS - 1
    for n, (first, size) in enumerate(((0, SPLIT), (SPLIT, CH - SPLIT))):
        x_kept(LAYERS - 1, end, STEPS - 1)[n].wait_recv()
        mix(LAYERS - 1, end, STEPS - 1, first, size)
        finish(end, first, size)

    for m in range(MATS):
        c0(m).wait_send()
        for k, j in pairs:
            c1(m, k, j).wait_send()
            c1f(m, k, j).wait_send()
            for p in parts_of(m):
                c2(m, k, j, p).wait_send()
            c2f(m, k, j).wait_send()
        for k in range(2):
            for p in range(4):
                c3(m, k, p).wait_send()
    for j in range(1, 4):
        h_halo(j).wait_send()

    @pl.when(mine == 0)
    def _():
        labels().wait_send()
        h_halo(0).wait_send()

    for c in range(CHUNKS):
        for j in range(1, 4):
            h_main(c, j).wait_send()
    for l in range(LAYERS):
        for c in range(CHUNKS):
            s = l * CHUNKS + c
            for copy in x_kept(l, c, s):
                copy.wait_send()
            send_sq(s).wait_send()
    pieces = [(HALO, CH - HALO)] + [(c * CH, CH) for c in range(1, CHUNKS - 1)]
    pieces += [(end * CH, SPLIT), (end * CH + SPLIT, CH - SPLIT)]
    for at, (start, size) in enumerate(pieces):
        keep_out(at, start, size).wait()
        for j in range(1, 4):
            send_out(at, j, start, size).wait_send()
            wait_out(at, j, start, size).wait_recv()


def body(stream, doc_ids, norm_gain, proj_in, mix_pool, pool_gain, proj_out):
    dma = pltpu.SemaphoreType.DMA
    steps = STEPS
    vmem = pl.BlockSpec(memory_space=pltpu.VMEM)
    hbm = pl.BlockSpec(memory_space=pl.ANY)
    return pl.pallas_call(
        kernel,
        out_shape=pltpu.VMEM((TOK, COLS), BF16),
        in_specs=[hbm, vmem, vmem, hbm, hbm, hbm, vmem],
        out_specs=vmem,
        scratch_shapes=[
            pltpu.VMEM((MATS, 2, 2, 4, 4, 64, COLS), BF16),
            pltpu.VMEM((4, HALO + PART, COLS), BF16),
            pltpu.VMEM((steps, CH, POOL), BF16),
            pltpu.VMEM((steps, CH, POOL), BF16),
            pltpu.VMEM((steps, 8, 128), F32),
            pltpu.VMEM((steps, 8, 128), F32),
            pltpu.VMEM((CH, WIDE), BF16),
            pltpu.VMEM((LEAD + CH, POOL), BF16),
            pltpu.VMEM((CH, POOL), BF16),
            pltpu.VMEM((128, 128), F32),
            pltpu.VMEM((CHUNKS, 4, CH, 128), BF16),
            pltpu.VMEM((CHUNKS, 4, CH, 128), F32),
            pltpu.VMEM((24, 128), jnp.int32),
            pltpu.VMEM((LAYERS, GROUPS, GROUP, GROUP), BF16),
            dma((MATS,)), dma((CHUNKS,)), dma((1,)), dma((CHUNKS + 1,)), dma((1,)),
            dma((MATS,)), dma((MATS,)),
            dma((MATS, 2, 2)), dma((MATS, 2, 2)), dma((MATS, 2, 2)), dma((MATS, 2, 2)),
            dma((MATS, 2, 2, 4)), dma((MATS, 2, 2, 4)), dma((MATS, 2, 2)), dma((MATS, 2, 2)),
            dma((MATS, 2, 4)), dma((MATS, 2, 4)),
            dma((CHUNKS, 4)), dma((CHUNKS, 4)), dma((4,)), dma((4,)), dma((1,)), dma((1,)),
            dma((steps + 5,)), dma((steps + 5,)), dma((steps,)), dma((steps,)),
            dma((CHUNKS + 1, 4)), dma((CHUNKS + 1, 4)),
        ],
        compiler_params=pltpu.CompilerParams(
            has_side_effects=True, collective_id=0, vmem_limit_bytes=56 * 1024 * 1024
        ),
        name="mixers",
    )(
        stream, doc_ids.reshape(16, 128), norm_gain, jnp.swapaxes(proj_in, 1, 2), proj_out,
        mix_pool, pool_gain,
    )


def solution(mesh):
    in_specs = (P("sp", "tp"), P("sp"), P(), P(None, "tp", "sp"), P(), P(), P(None, "sp", "tp"))
    out_specs = P("sp", "tp")
    return jax.shard_map(body, mesh=mesh, in_specs=in_specs, out_specs=out_specs, check_vma=False)
```

```python
import jax
import jax.numpy as jnp
from jax import lax
from jax.experimental import pallas as pl
from jax.experimental.pallas import tpu as pltpu
from jax.sharding import PartitionSpec as P

MESH = pl.DeviceIdType.MESH
F32 = jnp.float32
BF16 = jnp.bfloat16

D = 4096
POOL = 1024
GROUP = 128
GROUPS = POOL // GROUP
LAYERS = 3
MATS = 2 * LAYERS
TOK = 2048
COLS = 512
PART = TOK // 4
WIDE = 4 * COLS
HALO = 48
LEAD = 16
CHUNKS = 5
CH = (HALO + PART) // CHUNKS
WINDOWS = (2, 4, 8, 16)
STEPS = LAYERS * CHUNKS
SPLIT = 64
EPS = 1e-06


def kernel(
    stream, docs, norm_gain, w_in, w_out, mix_hbm, pool_gain, out,
    wbuf, hbuf, own, got, ssown, ssgot, gbuf, zbuf, mbuf, sqbuf, band, inv, ext, mix_pool,
    loc_w, loc_h, loc_hh, loc_o, loc_m,
    s0, r0, s1, r1, s1f, r1f, s2, r2, s2f, r2f, s3, r3,
    sh, rh, shh, rhh, sl, rl, sx, rx, sq, rq, so, ro,
):
    sp = lax.axis_index("sp")
    tp = lax.axis_index("tp")
    z, y = sp // 4, sp % 4
    x, core = tp // 2, tp % 2
    half, xl = x // 2, x % 2
    me = xl * 2 + core
    mine = (me + 2 * half) % 4

    def remote(src, dst, send, recv, device):
        return pltpu.make_async_remote_copy(
            src_ref=src, dst_ref=dst, send_sem=send, recv_sem=recv,
            device_id=device, device_id_type=MESH,
        )

    across = (sp, (2 * half + 1 - xl) * 2 + core)
    partner = (sp, (3 - x) * 2 + core)
    sibling = (sp, x * 2 + 1 - core)

    def along_y(d):
        return (z * 4 + (y + d + 4) % 4, tp)

    def along_z(d):
        return (((z + d + 4) % 4) * 4 + y, tp)

    first_axis = (along_y, along_z)
    second_axis = (along_z, along_y)
    steps = (1, -1)

    def shard(m, k, d):
        if k == 0:
            return wbuf.at[m, core, 0, z, (y + d + 4) % 4]
        return wbuf.at[m, core, 1, (z + d + 4) % 4, y]

    def plane(m, k, d, c=None):
        c = core if c is None else c
        if k == 0:
            return wbuf.at[m, c, 0, (z + d + 4) % 4]
        return wbuf.at[m, c, 1, :, (y + d + 4) % 4]

    def plane_half(m, k, d, which):
        part = pl.ds(2 * which, 2)
        if k == 0:
            return wbuf.at[m, core, 0, (z + d + 4) % 4, part]
        return wbuf.at[m, core, 1, part, (y + d + 4) % 4]

    pairs = [(k, j) for k in range(2) for j in range(2)]

    def c_local(m):
        source = w_in if m % 2 == 0 else w_out
        return pltpu.make_async_copy(source.at[m // 2], wbuf.at[m, core, xl, z, y], loc_w.at[m])

    def c0(m):
        return remote(wbuf.at[m, core, xl, z, y], wbuf.at[m, core, xl, z, y], s0.at[m], r0.at[m], across)

    def c1(m, k, j):
        return remote(shard(m, k, 0), shard(m, k, 0), s1.at[m, k, j], r1.at[m, k, j], first_axis[k](steps[j]))

    def c1f(m, k, j):
        ref = shard(m, k, -steps[j]).at[pl.ds(32 * j, 32)]
        return remote(ref, ref, s1f.at[m, k, j], r1f.at[m, k, j], first_axis[k](steps[j]))

    def c2(m, k, j, p):
        ref = shard(m, k, (0, -1, 1, 2)[p]) if m == 0 else plane(m, k, 0)
        return remote(ref, ref, s2.at[m, k, j, p], r2.at[m, k, j, p], second_axis[k](steps[j]))

    def c2f(m, k, j):
        ref = plane_half(m, k, -steps[j], j)
        return remote(ref, ref, s2f.at[m, k, j], r2f.at[m, k, j], second_axis[k](steps[j]))

    def c3(m, k, p):
        ref = plane(m, k, (0, -1, 1, 2)[p])
        return remote(ref, ref, s3.at[m, k, p], r3.at[m, k, p], sibling)

    def parts_of(m):
        return range(4 if m == 0 else 1)

    def row_start(m):
        c0(m).wait_recv()
        for k, j in pairs:
            c1(m, k, j).start()
        if m == 0:
            for k, j in pairs:
                c2(m, k, j, 0).start()

    def row_pass(m):
        for k, j in pairs:
            c1(m, k, j).wait_recv()
            c1f(m, k, j).start()
        if m == 0:
            for k, j in pairs:
                c2(m, k, 0, 1 + j).start()
                c2(m, k, 1, 1 + j).start()

    def row_end(m):
        for k in range(2):
            for j in range(2):
                c1f(m, k, j).wait_recv()
            for j in range(2):
                c2(m, k, j, 3 if m == 0 else 0).start()
            c3(m, k, 0).start()

    def plane_pass(m):
        for k, j in pairs:
            for p in parts_of(m):
                c2(m, k, j, p).wait_recv()
            c2f(m, k, j).start()
            c3(m, k, 1 + j).start()

    def plane_end(m):
        for k, j in pairs:
            c2f(m, k, j).wait_recv()
        for k in range(2):
            c3(m, k, 3).start()

    def weights_ready(m):
        for k in range(2):
            for p in range(4):
                c3(m, k, p).wait_recv()

    def peer(j):
        return (me + j) % 4

    def rows_of(c):
        return (HALO, CH - HALO) if c == 0 else (CH * c, CH)

    def h_main(c, j):
        to = peer(j)
        start, size = rows_of(c)
        base = ((to + 2 * half) % 4) * PART + start - HALO
        return remote(
            stream.at[pl.ds(pl.multiple_of(base, 16), size)], hbuf.at[me, pl.ds(start, size)],
            sh.at[c, j], rh.at[c, me], (sp, 4 * half + to),
        )

    def h_main_wait(c, j):
        start, size = rows_of(c)
        ref = hbuf.at[peer(j), pl.ds(start, size)]
        return remote(ref, ref, sh.at[c, j], rh.at[c, peer(j)], (sp, 4 * half + peer(j)))

    def h_main_local(c):
        start, size = rows_of(c)
        base = mine * PART + start - HALO
        return pltpu.make_async_copy(
            stream.at[pl.ds(pl.multiple_of(base, 16), size)], hbuf.at[me, pl.ds(start, size)], loc_h.at[c]
        )

    def h_halo(j):
        to = peer(j)
        quarter = (to + 2 * half) % 4
        base = (quarter * PART + TOK - HALO) % TOK
        to_sp = (sp + 1 - (quarter + 3) // 4) % 16
        return remote(
            stream.at[pl.ds(pl.multiple_of(base, 16), HALO)], hbuf.at[me, pl.ds(0, HALO)],
            shh.at[j], rhh.at[me], (to_sp, 4 * half + to),
        )

    def h_halo_wait(j):
        ref = hbuf.at[peer(j), pl.ds(0, HALO)]
        return remote(ref, ref, shh.at[j], rhh.at[peer(j)], (sp, 4 * half + peer(3)))

    def h_halo_local():
        base = (mine * PART + TOK - HALO) % TOK
        return pltpu.make_async_copy(
            stream.at[pl.ds(pl.multiple_of(base, 16), HALO)], hbuf.at[me, pl.ds(0, HALO)], loc_hh.at[0]
        )

    def labels():
        return remote(docs.at[pl.ds(15, 1)], ext.at[pl.ds(7, 1)], sl.at[0], rl.at[0], ((sp + 1) % 16, tp))

    mix_copy = pltpu.make_async_copy(mix_hbm, mix_pool, loc_m.at[0])
    for m in range(MATS):
        c_local(m).start()
    mix_copy.start()
    greeted = [across, partner, sibling, (sp, (2 * half + 1 - xl) * 2 + 1 - core)]
    greeted += [along_y(1), along_y(-1), along_z(1), along_z(-1)]
    barrier = pltpu.get_barrier_semaphore()
    for device in greeted:
        pl.semaphore_signal(barrier, inc=1, device_id=device, device_id_type=MESH)

    @pl.when(mine == 0)
    def _():
        for j in range(4):
            device = ((sp + 15) % 16, 4 * half + peer(j))
            pl.semaphore_signal(barrier, inc=1, device_id=device, device_id_type=MESH)

    pl.semaphore_wait(barrier, len(greeted) + 1)

    for m in range(3):
        c_local(m).wait()
        c0(m).start()
    for j in range(1, 4):
        h_halo(j).start()

    @pl.when(mine == 0)
    def _():
        labels().start()
        h_halo(0).start()

    @pl.when(mine != 0)
    def _():
        h_halo_local().start()

    for c in range(CHUNKS):
        h_main_local(c).start()
        for j in range(1, 4):
            h_main(c, j).start()
        if c == 2:
            c_local(3).wait()
            c0(3).start()
    for m in range(4, MATS):
        c_local(m).wait()
        c0(m).start()

    row_start(0)

    zbuf[...] = jnp.zeros_like(zbuf)
    sqbuf[...] = jnp.zeros_like(sqbuf)
    for l in range(1, LAYERS):
        got[l * CHUNKS, 0 : LEAD * l, :] = jnp.zeros((LEAD * l, POOL), BF16)
    ext[8:24, :] = docs[...]

    @pl.when(mine == 0)
    def _():
        labels().wait_recv()

    label_rows = []
    for k in range(5):
        row = (ext[pl.ds(4 * mine + 7 + k, 1), :] + 1).astype(F32)
        if k == 0:
            row = jnp.where(jnp.logical_and(sp == 0, mine == 0), jnp.zeros_like(row), row)
        label_rows.append(row)
    t_id = lax.broadcasted_iota(jnp.int32, (128, 128), 0)
    s_id = lax.broadcasted_iota(jnp.int32, (128, 128), 1)
    back = t_id - s_id
    lane = lax.broadcasted_iota(jnp.int32, (1, 128), 1)
    for c in range(CHUNKS):
        first, off = divmod(128 - HALO - LEAD + CH * c, 128)
        if off == 0:
            window = label_rows[first]
        else:
            window = jnp.where(
                lane < 128 - off,
                pltpu.roll(label_rows[first], 128 - off, 1),
                pltpu.roll(label_rows[first + 1], 128 - off, 1),
            )
        across_lanes = jnp.broadcast_to(window, (128, 128))
        same = jnp.logical_and(across_lanes == across_lanes.T, back >= 0)
        for i, w in enumerate(WINDOWS):
            member = jnp.where(jnp.logical_and(same, back < w), 1.0, 0.0).astype(F32)
            count = jnp.sum(member, axis=1, keepdims=True)
            band[c, i] = member[LEAD:].astype(BF16)
            inv[c, i] = jnp.broadcast_to(1.0 / count, (128, 128))[LEAD:]

    row_pass(0)
    row_end(0)
    row_start(1)
    row_start(2)
    plane_pass(0)
    row_pass(1)
    row_pass(2)
    row_start(3)
    plane_end(0)
    row_end(1)
    weights_ready(0)
    row_end(2)

    def rows_at(c):
        return pl.ds(pl.multiple_of(c * CH, 16), CH)

    def squares_of(wide):
        total = None
        for k in range(COLS // 128):
            piece = wide[:, k * 128 : (k + 1) * 128]
            total = piece * piece if total is None else total + piece * piece
        return total

    def gain_of(l, b):
        at = pl.ds(pl.multiple_of(half * WIDE + b * COLS, COLS), COLS)
        return norm_gain[l : l + 1, at].astype(F32)

    def send_x(s, at, rows=(0, CH), lanes=(0, POOL)):
        index = (s, pl.ds(*rows), pl.ds(*lanes))
        return remote(own.at[index], got.at[index], sx.at[at], rx.at[at], partner)

    def x_first(n):
        return send_x(0, STEPS + 1 + n, lanes=(n * 256, 256))

    def x_kept(l, c, s):
        if c == 0 and l > 0:
            return [send_x(s, s, rows=(LEAD * l, CH - LEAD * l))]
        if c == CHUNKS - 1 and l == LAYERS - 1:
            return [send_x(s, s, rows=(0, SPLIT)), send_x(s, STEPS, rows=(SPLIT, CH - SPLIT))]
        if c == 0:
            return [x_first(n) for n in range(4)]
        return [send_x(s, s)]

    def on_x(l, c, s, act):
        special = [0, CHUNKS - 1] if l == LAYERS - 1 else [0]
        plain = c != 0
        for k in special:

            @pl.when(c == k)
            def _(k=k):
                for copy in x_kept(l, k, s):
                    act(copy)

            plain = jnp.logical_and(plain, c != k)

        @pl.when(plain)
        def _():
            act(send_x(s, s))

    def send_sq(s):
        return remote(ssown.at[s], ssgot.at[s], sq.at[s], rq.at[s], partner)

    def share_squares(s, squares):
        sqbuf[0:CH, :] = squares
        ssown[s] = jnp.broadcast_to(jnp.sum(sqbuf[...].T, axis=0, keepdims=True), (8, 128))
        send_sq(s).start()

    def project(l, chunks):
        rows = slice(chunks[0] * CH, (chunks[-1] + 1) * CH)
        for n in range(4):
            rhs = jnp.concatenate(
                [wbuf[2 * l, b % 2, b // 2, n].reshape(256, COLS) for b in range(4)], axis=1
            )
            part = lax.dot_general(
                gbuf[rows, :], rhs, (((1,), (1,)), ((), ())), preferred_element_type=F32
            ).astype(BF16)
            for k, c in enumerate(chunks):
                own[l * CHUNKS + c, :, n * 256 : (n + 1) * 256] = part[k * CH : (k + 1) * CH]
                if l == 0 and c == 0:
                    x_first(n).start()
        for c in chunks:
            if l > 0 or c > 0:
                for copy in x_kept(l, c, l * CHUNKS + c):
                    copy.start()

    def mix(l, c, s, first=0, size=CH):
        rows = slice(first, first + size)
        here = slice(LEAD + first, LEAD + first + size)
        if first == 0:
            send_sq(s).wait_recv()
            zbuf[0:LEAD, :] = zbuf[CH : CH + LEAD, :]
        scale = lax.rsqrt((ssown[s] + ssgot[s]) / D + EPS)[0:1]
        scale = jnp.broadcast_to(scale, (128, 128)).T[rows]
        for i in range(GROUPS):
            at = slice(i * GROUP, (i + 1) * GROUP)
            summed = own[s, rows, at].astype(F32) + got[s, rows, at].astype(F32)
            zbuf[here, at] = (summed * scale).astype(BF16)
        for i in range(GROUPS):
            at = slice(i * GROUP, (i + 1) * GROUP)
            total = jnp.dot(band[c, i % 4, rows], zbuf[:, at], preferred_element_type=F32)
            pooled = (total * inv[c, i % 4, rows] - zbuf[here, at].astype(F32)).astype(BF16)
            blended = jnp.dot(pooled, mix_pool[l, i], preferred_element_type=F32)
            mbuf[rows, at] = (blended * pool_gain[l : l + 1, at].astype(F32)).astype(BF16)

    def update(l, c):
        rows = rows_at(c)
        squares = None
        for b in range(4):
            weights = wbuf[2 * l + 1, b % 2, b // 2].reshape(POOL, COLS)
            change = jnp.dot(mbuf[...], weights, preferred_element_type=F32)
            new = (hbuf[b, rows, :].astype(F32) + change).astype(BF16)
            hbuf[b, rows, :] = new
            wide = new.astype(F32)
            squares = squares_of(wide) if squares is None else squares + squares_of(wide)
            gbuf[rows, b * COLS : (b + 1) * COLS] = (wide * gain_of(l + 1, b)).astype(BF16)
        return squares

    def finish(c, first=0, size=CH):
        for j in (2, 3, 1, 0):
            b = peer(j)
            weights = wbuf[MATS - 1, b % 2, b // 2].reshape(POOL, COLS)
            change = jnp.dot(mbuf[first : first + size], weights, preferred_element_type=F32)
            rows = pl.ds(pl.multiple_of(c * CH + first, 16), size)
            hbuf[b, rows, :] = (hbuf[b, rows, :].astype(F32) + change).astype(BF16)
            if isinstance(c, int):
                at = c + (first > 0)
                (send_out(at, j, c * CH + first, size) if j else keep_out(at, c * CH + first, size)).start()
                continue
            for start, size_ in ((HALO, CH - HALO), (pl.multiple_of(c * CH, 16), CH)):

                @pl.when(c == 0 if size_ < CH else c != 0)
                def _(j=j, start=start, size_=size_):
                    (send_out(c, j, start, size_) if j else keep_out(c, start, size_)).start()

    def wait_rows(c):
        h_main_local(c).wait()
        for j in range(1, 4):
            h_main_wait(c, j).wait_recv()

    @pl.when(mine == 0)
    def _():
        h_halo_wait(0).wait_recv()

    @pl.when(mine != 0)
    def _():
        h_halo_local().wait()

    for j in range(1, 4):
        h_halo_wait(j).wait_recv()

    def enter(c, carry):
        for k in range(CHUNKS):

            @pl.when(c == k)
            def _(k=k):
                wait_rows(k)

        rows = rows_at(c)
        squares = None
        for b in range(4):
            wide = hbuf[b, rows, :].astype(F32)
            squares = squares_of(wide) if squares is None else squares + squares_of(wide)
            gbuf[rows, b * COLS : (b + 1) * COLS] = (wide * gain_of(0, b)).astype(BF16)
        share_squares(c, squares)

        @pl.when(c == 2)
        def _():
            project(0, (0, 1, 2))
            row_pass(3)

        @pl.when(c == 3)
        def _():
            plane_pass(1)

        @pl.when(c == 4)
        def _():
            project(0, (3, 4))

        return carry

    lax.fori_loop(0, CHUNKS, enter, 0)

    row_start(4)
    plane_pass(2)
    row_end(3)
    plane_end(1)
    weights_ready(1)
    row_pass(4)
    row_start(5)
    plane_end(2)
    weights_ready(2)

    def out_rows(quarter, start, size):
        base = pl.multiple_of(quarter * PART + start - HALO, 16)
        return pl.ds(start, size), pl.ds(base, size)

    def send_out(at, j, start, size):
        here, there = out_rows(mine, start, size)
        to = peer(j)
        return remote(
            hbuf.at[to, here], out.at[there], so.at[at, j], ro.at[at, me], (sp, 4 * half + to)
        )

    def keep_out(at, start, size):
        here, there = out_rows(mine, start, size)
        return pltpu.make_async_copy(hbuf.at[me, here], out.at[there], loc_o.at[at])

    def wait_out(at, j, start, size):
        frm = peer(j)
        _, there = out_rows((frm + 2 * half) % 4, start, size)
        ref = out.at[there]
        return remote(ref, ref, so.at[at, j], ro.at[at, frm], (sp, 4 * half + frm))

    mix_copy.wait()
    for l in range(LAYERS):
        last = l == LAYERS - 1
        if l == 1:
            plane_end(3)
            weights_ready(3)
            plane_pass(4)
            row_end(5)
            plane_end(4)
            weights_ready(4)
        if l == 2:
            plane_end(5)
            weights_ready(5)

        def one(c, carry, l=l, last=last):
            s = l * CHUNKS + c
            on_x(l, c, s, lambda copy: copy.wait_recv())
            mix(l, c, s)
            if last:
                finish(c)
            else:
                share_squares(s + CHUNKS, update(l, c))

                @pl.when(c == 1)
                def _():
                    project(l + 1, (0, 1))
                    plane_pass(3 if l == 0 else 5)

                if l == 0:

                    @pl.when(c == 2)
                    def _():
                        row_end(4)
                        row_pass(5)

                @pl.when(c == 4)
                def _():
                    project(l + 1, (2, 3, 4))

            return carry

        lax.fori_loop(0, CHUNKS - 1 if last else CHUNKS, one, 0)

    end = CHUNKS - 1
    for n, (first, size) in enumerate(((0, SPLIT), (SPLIT, CH - SPLIT))):
        x_kept(LAYERS - 1, end, STEPS - 1)[n].wait_recv()
        mix(LAYERS - 1, end, STEPS - 1, first, size)
        finish(end, first, size)

    for m in range(MATS):
        c0(m).wait_send()
        for k, j in pairs:
            c1(m, k, j).wait_send()
            c1f(m, k, j).wait_send()
            for p in parts_of(m):
                c2(m, k, j, p).wait_send()
            c2f(m, k, j).wait_send()
        for k in range(2):
            for p in range(4):
                c3(m, k, p).wait_send()
    for j in range(1, 4):
        h_halo(j).wait_send()

    @pl.when(mine == 0)
    def _():
        labels().wait_send()
        h_halo(0).wait_send()

    for c in range(CHUNKS):
        for j in range(1, 4):
            h_main(c, j).wait_send()
    for l in range(LAYERS):
        for c in range(CHUNKS):
            s = l * CHUNKS + c
            for copy in x_kept(l, c, s):
                copy.wait_send()
            send_sq(s).wait_send()
    pieces = [(HALO, CH - HALO)] + [(c * CH, CH) for c in range(1, CHUNKS - 1)]
    pieces += [(end * CH, SPLIT), (end * CH + SPLIT, CH - SPLIT)]
    for at, (start, size) in enumerate(pieces):
        keep_out(at, start, size).wait()
        for j in range(1, 4):
            send_out(at, j, start, size).wait_send()
            wait_out(at, j, start, size).wait_recv()


def body(stream, doc_ids, norm_gain, proj_in, mix_pool, pool_gain, proj_out):
    dma = pltpu.SemaphoreType.DMA
    steps = STEPS
    vmem = pl.BlockSpec(memory_space=pltpu.VMEM)
    hbm = pl.BlockSpec(memory_space=pl.ANY)
    return pl.pallas_call(
        kernel,
        out_shape=pltpu.VMEM((TOK, COLS), BF16),
        in_specs=[hbm, vmem, vmem, hbm, hbm, hbm, vmem],
        out_specs=vmem,
        scratch_shapes=[
            pltpu.VMEM((MATS, 2, 2, 4, 4, 64, COLS), BF16),
            pltpu.VMEM((4, HALO + PART, COLS), BF16),
            pltpu.VMEM((steps, CH, POOL), BF16),
            pltpu.VMEM((steps, CH, POOL), BF16),
            pltpu.VMEM((steps, 8, 128), F32),
            pltpu.VMEM((steps, 8, 128), F32),
            pltpu.VMEM((CHUNKS * CH, WIDE), BF16),
            pltpu.VMEM((LEAD + CH, POOL), BF16),
            pltpu.VMEM((CH, POOL), BF16),
            pltpu.VMEM((128, 128), F32),
            pltpu.VMEM((CHUNKS, 4, CH, 128), BF16),
            pltpu.VMEM((CHUNKS, 4, CH, 128), F32),
            pltpu.VMEM((24, 128), jnp.int32),
            pltpu.VMEM((LAYERS, GROUPS, GROUP, GROUP), BF16),
            dma((MATS,)), dma((CHUNKS,)), dma((1,)), dma((CHUNKS + 1,)), dma((1,)),
            dma((MATS,)), dma((MATS,)),
            dma((MATS, 2, 2)), dma((MATS, 2, 2)), dma((MATS, 2, 2)), dma((MATS, 2, 2)),
            dma((MATS, 2, 2, 4)), dma((MATS, 2, 2, 4)), dma((MATS, 2, 2)), dma((MATS, 2, 2)),
            dma((MATS, 2, 4)), dma((MATS, 2, 4)),
            dma((CHUNKS, 4)), dma((CHUNKS, 4)), dma((4,)), dma((4,)), dma((1,)), dma((1,)),
            dma((steps + 5,)), dma((steps + 5,)), dma((steps,)), dma((steps,)),
            dma((CHUNKS + 1, 4)), dma((CHUNKS + 1, 4)),
        ],
        compiler_params=pltpu.CompilerParams(
            has_side_effects=True, collective_id=0, vmem_limit_bytes=56 * 1024 * 1024
        ),
        name="mixers",
    )(
        stream, doc_ids.reshape(16, 128), norm_gain, jnp.swapaxes(proj_in, 1, 2), proj_out,
        mix_pool, pool_gain,
    )


def solution(mesh):
    in_specs = (P("sp", "tp"), P("sp"), P(), P(None, "tp", "sp"), P(), P(), P(None, "sp", "tp"))
    out_specs = P("sp", "tp")
    return jax.shard_map(body, mesh=mesh, in_specs=in_specs, out_specs=out_specs, check_vma=False)
```

```python
import jax
import jax.numpy as jnp
from jax import lax
from jax.experimental import pallas as pl
from jax.experimental.pallas import tpu as pltpu
from jax.sharding import PartitionSpec as P

MESH = pl.DeviceIdType.MESH
F32 = jnp.float32
BF16 = jnp.bfloat16

D = 4096
POOL = 1024
GROUP = 128
GROUPS = POOL // GROUP
LAYERS = 3
MATS = 2 * LAYERS
TOK = 2048
COLS = 512
PART = TOK // 4
WIDE = 4 * COLS
HALO = 48
LEAD = 16
CHUNKS = 5
CH = (HALO + PART) // CHUNKS
WINDOWS = (2, 4, 8, 16)
STEPS = LAYERS * CHUNKS
SPLIT = 64
EPS = 1e-06


def kernel(
    stream, docs, norm_gain, w_in, w_out, mix_hbm, pool_gain, out,
    wbuf, hbuf, own, got, ssown, ssgot, gbuf, zbuf, mbuf, sqbuf, band, inv, ext, mix_pool,
    loc_w, loc_h, loc_hh, loc_o, loc_m,
    s0, r0, s1, r1, s1f, r1f, s2, r2, s2f, r2f, s3, r3,
    sh, rh, shh, rhh, sl, rl, sx, rx, sq, rq, so, ro,
):
    sp = lax.axis_index("sp")
    tp = lax.axis_index("tp")
    z, y = sp // 4, sp % 4
    x, core = tp // 2, tp % 2
    half, xl = x // 2, x % 2
    me = xl * 2 + core
    mine = (me + 2 * half) % 4

    def remote(src, dst, send, recv, device):
        return pltpu.make_async_remote_copy(
            src_ref=src, dst_ref=dst, send_sem=send, recv_sem=recv,
            device_id=device, device_id_type=MESH,
        )

    across = (sp, (2 * half + 1 - xl) * 2 + core)
    partner = (sp, (3 - x) * 2 + core)
    sibling = (sp, x * 2 + 1 - core)

    def along_y(d):
        return (z * 4 + (y + d + 4) % 4, tp)

    def along_z(d):
        return (((z + d + 4) % 4) * 4 + y, tp)

    first_axis = (along_y, along_z)
    second_axis = (along_z, along_y)
    steps = (1, -1)

    def shard(m, k, d):
        if k == 0:
            return wbuf.at[m, core, 0, z, (y + d + 4) % 4]
        return wbuf.at[m, core, 1, (z + d + 4) % 4, y]

    def plane(m, k, d, c=None):
        c = core if c is None else c
        if k == 0:
            return wbuf.at[m, c, 0, (z + d + 4) % 4]
        return wbuf.at[m, c, 1, :, (y + d + 4) % 4]

    def plane_half(m, k, d, which):
        part = pl.ds(2 * which, 2)
        if k == 0:
            return wbuf.at[m, core, 0, (z + d + 4) % 4, part]
        return wbuf.at[m, core, 1, part, (y + d + 4) % 4]

    pairs = [(k, j) for k in range(2) for j in range(2)]

    def c_local(m):
        source = w_in if m % 2 == 0 else w_out
        return pltpu.make_async_copy(source.at[m // 2], wbuf.at[m, core, xl, z, y], loc_w.at[m])

    def c0(m):
        return remote(wbuf.at[m, core, xl, z, y], wbuf.at[m, core, xl, z, y], s0.at[m], r0.at[m], across)

    def c1(m, k, j):
        return remote(shard(m, k, 0), shard(m, k, 0), s1.at[m, k, j], r1.at[m, k, j], first_axis[k](steps[j]))

    def c1f(m, k, j):
        ref = shard(m, k, -steps[j]).at[pl.ds(32 * j, 32)]
        return remote(ref, ref, s1f.at[m, k, j], r1f.at[m, k, j], first_axis[k](steps[j]))

    def c2(m, k, j, p):
        ref = shard(m, k, (0, -1, 1, 2)[p]) if m == 0 else plane(m, k, 0)
        return remote(ref, ref, s2.at[m, k, j, p], r2.at[m, k, j, p], second_axis[k](steps[j]))

    def c2f(m, k, j):
        ref = plane_half(m, k, -steps[j], j)
        return remote(ref, ref, s2f.at[m, k, j], r2f.at[m, k, j], second_axis[k](steps[j]))

    def c3(m, k, p):
        ref = plane(m, k, (0, -1, 1, 2)[p])
        return remote(ref, ref, s3.at[m, k, p], r3.at[m, k, p], sibling)

    def parts_of(m):
        return range(4 if m == 0 else 1)

    def row_start(m):
        c0(m).wait_recv()
        for k, j in pairs:
            c1(m, k, j).start()
        if m == 0:
            for k, j in pairs:
                c2(m, k, j, 0).start()

    def row_pass(m):
        for k, j in pairs:
            c1(m, k, j).wait_recv()
            c1f(m, k, j).start()
        if m == 0:
            for k, j in pairs:
                c2(m, k, 0, 1 + j).start()
                c2(m, k, 1, 1 + j).start()

    def row_end(m):
        for k in range(2):
            for j in range(2):
                c1f(m, k, j).wait_recv()
            for j in range(2):
                c2(m, k, j, 3 if m == 0 else 0).start()
            c3(m, k, 0).start()

    def plane_pass(m):
        for k, j in pairs:
            for p in parts_of(m):
                c2(m, k, j, p).wait_recv()
            c2f(m, k, j).start()
            c3(m, k, 1 + j).start()

    def plane_end(m):
        for k, j in pairs:
            c2f(m, k, j).wait_recv()
        for k in range(2):
            c3(m, k, 3).start()

    def weights_ready(m):
        for k in range(2):
            for p in range(4):
                c3(m, k, p).wait_recv()

    def peer(j):
        return (me + j) % 4

    def rows_of(c):
        return (HALO, CH - HALO) if c == 0 else (CH * c, CH)

    def h_main(c, j):
        to = peer(j)
        start, size = rows_of(c)
        base = ((to + 2 * half) % 4) * PART + start - HALO
        return remote(
            stream.at[pl.ds(pl.multiple_of(base, 16), size)], hbuf.at[me, pl.ds(start, size)],
            sh.at[c, j], rh.at[c, me], (sp, 4 * half + to),
        )

    def h_main_wait(c, j):
        start, size = rows_of(c)
        ref = hbuf.at[peer(j), pl.ds(start, size)]
        return remote(ref, ref, sh.at[c, j], rh.at[c, peer(j)], (sp, 4 * half + peer(j)))

    def h_main_local(c):
        start, size = rows_of(c)
        base = mine * PART + start - HALO
        return pltpu.make_async_copy(
            stream.at[pl.ds(pl.multiple_of(base, 16), size)], hbuf.at[me, pl.ds(start, size)], loc_h.at[c]
        )

    def h_halo(j):
        to = peer(j)
        quarter = (to + 2 * half) % 4
        base = (quarter * PART + TOK - HALO) % TOK
        to_sp = (sp + 1 - (quarter + 3) // 4) % 16
        return remote(
            stream.at[pl.ds(pl.multiple_of(base, 16), HALO)], hbuf.at[me, pl.ds(0, HALO)],
            shh.at[j], rhh.at[me], (to_sp, 4 * half + to),
        )

    def h_halo_wait(j):
        ref = hbuf.at[peer(j), pl.ds(0, HALO)]
        return remote(ref, ref, shh.at[j], rhh.at[peer(j)], (sp, 4 * half + peer(3)))

    def h_halo_local():
        base = (mine * PART + TOK - HALO) % TOK
        return pltpu.make_async_copy(
            stream.at[pl.ds(pl.multiple_of(base, 16), HALO)], hbuf.at[me, pl.ds(0, HALO)], loc_hh.at[0]
        )

    def labels():
        return remote(docs.at[pl.ds(15, 1)], ext.at[pl.ds(7, 1)], sl.at[0], rl.at[0], ((sp + 1) % 16, tp))

    mix_copy = pltpu.make_async_copy(mix_hbm, mix_pool, loc_m.at[0])
    for m in range(MATS):
        c_local(m).start()
    mix_copy.start()
    greeted = [across, partner, sibling, (sp, (2 * half + 1 - xl) * 2 + 1 - core)]
    greeted += [along_y(1), along_y(-1), along_z(1), along_z(-1)]
    barrier = pltpu.get_barrier_semaphore()
    for device in greeted:
        pl.semaphore_signal(barrier, inc=1, device_id=device, device_id_type=MESH)

    @pl.when(mine == 0)
    def _():
        for j in range(4):
            device = ((sp + 15) % 16, 4 * half + peer(j))
            pl.semaphore_signal(barrier, inc=1, device_id=device, device_id_type=MESH)

    pl.semaphore_wait(barrier, len(greeted) + 1)

    for m in range(3):
        c_local(m).wait()
        c0(m).start()
    for j in range(1, 4):
        h_halo(j).start()

    @pl.when(mine == 0)
    def _():
        labels().start()
        h_halo(0).start()

    @pl.when(mine != 0)
    def _():
        h_halo_local().start()

    for c in range(CHUNKS):
        h_main_local(c).start()
        for j in range(1, 4):
            h_main(c, j).start()
        if c == 2:
            c_local(3).wait()
            c0(3).start()
    for m in range(4, MATS):
        c_local(m).wait()
        c0(m).start()

    row_start(0)

    zbuf[...] = jnp.zeros_like(zbuf)
    sqbuf[...] = jnp.zeros_like(sqbuf)
    for l in range(1, LAYERS):
        got[l * CHUNKS, 0 : LEAD * l, :] = jnp.zeros((LEAD * l, POOL), BF16)
    ext[8:24, :] = docs[...]

    @pl.when(mine == 0)
    def _():
        labels().wait_recv()

    label_rows = []
    for k in range(5):
        row = (ext[pl.ds(4 * mine + 7 + k, 1), :] + 1).astype(F32)
        if k == 0:
            row = jnp.where(jnp.logical_and(sp == 0, mine == 0), jnp.zeros_like(row), row)
        label_rows.append(row)
    t_id = lax.broadcasted_iota(jnp.int32, (128, 128), 0)
    s_id = lax.broadcasted_iota(jnp.int32, (128, 128), 1)
    back = t_id - s_id
    lane = lax.broadcasted_iota(jnp.int32, (1, 128), 1)
    for c in range(CHUNKS):
        first, off = divmod(128 - HALO - LEAD + CH * c, 128)
        if off == 0:
            window = label_rows[first]
        else:
            window = jnp.where(
                lane < 128 - off,
                pltpu.roll(label_rows[first], 128 - off, 1),
                pltpu.roll(label_rows[first + 1], 128 - off, 1),
            )
        across_lanes = jnp.broadcast_to(window, (128, 128))
        same = jnp.logical_and(across_lanes == across_lanes.T, back >= 0)
        for i, w in enumerate(WINDOWS):
            member = jnp.where(jnp.logical_and(same, back < w), 1.0, 0.0).astype(F32)
            count = jnp.sum(member, axis=1, keepdims=True)
            band[c, i] = member[LEAD:].astype(BF16)
            inv[c, i] = jnp.broadcast_to(1.0 / count, (128, 128))[LEAD:]

    row_pass(0)
    row_end(0)
    row_start(1)
    row_start(2)
    plane_pass(0)
    row_pass(1)
    row_pass(2)
    row_start(3)
    plane_end(0)
    row_end(1)
    weights_ready(0)
    row_end(2)

    def rows_at(c):
        return pl.ds(pl.multiple_of(c * CH, 16), CH)

    def squares_of(wide):
        total = None
        for k in range(COLS // 128):
            piece = wide[:, k * 128 : (k + 1) * 128]
            total = piece * piece if total is None else total + piece * piece
        return total

    def gain_of(l, b):
        at = pl.ds(pl.multiple_of(half * WIDE + b * COLS, COLS), COLS)
        return norm_gain[l : l + 1, at].astype(F32)

    def send_x(s, at, rows=(0, CH), lanes=(0, POOL)):
        index = (s, pl.ds(*rows), pl.ds(*lanes))
        return remote(own.at[index], got.at[index], sx.at[at], rx.at[at], partner)

    def x_first(n):
        return send_x(0, STEPS + 1 + n, lanes=(n * 256, 256))

    def x_kept(l, c, s):
        if c == 0 and l > 0:
            return [send_x(s, s, rows=(LEAD * l, CH - LEAD * l))]
        if c == CHUNKS - 1 and l == LAYERS - 1:
            return [send_x(s, s, rows=(0, SPLIT)), send_x(s, STEPS, rows=(SPLIT, CH - SPLIT))]
        if c == 0:
            return [x_first(n) for n in range(4)]
        return [send_x(s, s)]

    def on_x(l, c, s, act):
        special = [0, CHUNKS - 1] if l == LAYERS - 1 else [0]
        plain = c != 0
        for k in special:

            @pl.when(c == k)
            def _(k=k):
                for copy in x_kept(l, k, s):
                    act(copy)

            plain = jnp.logical_and(plain, c != k)

        @pl.when(plain)
        def _():
            act(send_x(s, s))

    def send_sq(s):
        return remote(ssown.at[s], ssgot.at[s], sq.at[s], rq.at[s], partner)

    def share_squares(s, squares):
        sqbuf[0:CH, :] = squares
        ssown[s] = jnp.broadcast_to(jnp.sum(sqbuf[...].T, axis=0, keepdims=True), (8, 128))
        send_sq(s).start()

    def project(l, chunks):
        rows = slice(chunks[0] * CH, (chunks[-1] + 1) * CH)
        for n in range(4):
            rhs = jnp.concatenate(
                [wbuf[2 * l, b % 2, b // 2, n].reshape(256, COLS) for b in range(4)], axis=1
            )
            part = lax.dot_general(
                gbuf[rows, :], rhs, (((1,), (1,)), ((), ())), preferred_element_type=F32
            ).astype(BF16)
            for k, c in enumerate(chunks):
                own[l * CHUNKS + c, :, n * 256 : (n + 1) * 256] = part[k * CH : (k + 1) * CH]
                if l == 0 and c == 0:
                    x_first(n).start()
        for c in chunks:
            if l > 0 or c > 0:
                for copy in x_kept(l, c, l * CHUNKS + c):
                    copy.start()

    def mix(l, c, s, first=0, size=CH):
        rows = slice(first, first + size)
        here = slice(LEAD + first, LEAD + first + size)
        if first == 0:
            send_sq(s).wait_recv()
            zbuf[0:LEAD, :] = zbuf[CH : CH + LEAD, :]
        scale = lax.rsqrt((ssown[s] + ssgot[s]) / D + EPS)[0:1]
        scale = jnp.broadcast_to(scale, (128, 128)).T[rows]
        for i in range(GROUPS):
            at = slice(i * GROUP, (i + 1) * GROUP)
            summed = own[s, rows, at].astype(F32) + got[s, rows, at].astype(F32)
            zbuf[here, at] = (summed * scale).astype(BF16)
        for i in range(GROUPS):
            at = slice(i * GROUP, (i + 1) * GROUP)
            total = jnp.dot(band[c, i % 4, rows], zbuf[:, at], preferred_element_type=F32)
            pooled = (total * inv[c, i % 4, rows] - zbuf[here, at].astype(F32)).astype(BF16)
            blended = jnp.dot(pooled, mix_pool[l, i], preferred_element_type=F32)
            mbuf[rows, at] = (blended * pool_gain[l : l + 1, at].astype(F32)).astype(BF16)

    def update(l, c):
        rows = rows_at(c)
        squares = None
        for b in range(4):
            weights = wbuf[2 * l + 1, b % 2, b // 2].reshape(POOL, COLS)
            change = jnp.dot(mbuf[...], weights, preferred_element_type=F32)
            new = (hbuf[b, rows, :].astype(F32) + change).astype(BF16)
            hbuf[b, rows, :] = new
            wide = new.astype(F32)
            squares = squares_of(wide) if squares is None else squares + squares_of(wide)
            gbuf[rows, b * COLS : (b + 1) * COLS] = (wide * gain_of(l + 1, b)).astype(BF16)
        return squares

    def finish(c, first=0, size=CH):
        for j in (2, 3, 1, 0):
            b = peer(j)
            weights = wbuf[MATS - 1, b % 2, b // 2].reshape(POOL, COLS)
            change = jnp.dot(mbuf[first : first + size], weights, preferred_element_type=F32)
            rows = pl.ds(pl.multiple_of(c * CH + first, 16), size)
            hbuf[b, rows, :] = (hbuf[b, rows, :].astype(F32) + change).astype(BF16)
            if isinstance(c, int):
                at = c + (first > 0)
                (send_out(at, j, c * CH + first, size) if j else keep_out(at, c * CH + first, size)).start()
                continue
            for start, size_ in ((HALO, CH - HALO), (pl.multiple_of(c * CH, 16), CH)):

                @pl.when(c == 0 if size_ < CH else c != 0)
                def _(j=j, start=start, size_=size_):
                    (send_out(c, j, start, size_) if j else keep_out(c, start, size_)).start()

    def wait_rows(c):
        h_main_local(c).wait()
        for j in range(1, 4):
            h_main_wait(c, j).wait_recv()

    @pl.when(mine == 0)
    def _():
        h_halo_wait(0).wait_recv()

    @pl.when(mine != 0)
    def _():
        h_halo_local().wait()

    for j in range(1, 4):
        h_halo_wait(j).wait_recv()

    def enter(c, carry):
        for k in range(CHUNKS):

            @pl.when(c == k)
            def _(k=k):
                wait_rows(k)

        rows = rows_at(c)
        squares = None
        for b in range(4):
            wide = hbuf[b, rows, :].astype(F32)
            squares = squares_of(wide) if squares is None else squares + squares_of(wide)
            gbuf[rows, b * COLS : (b + 1) * COLS] = (wide * gain_of(0, b)).astype(BF16)
        share_squares(c, squares)

        @pl.when(c == 1)
        def _():
            project(0, (0, 1))

        @pl.when(c == 2)
        def _():
            project(0, (2,))
            row_pass(3)

        @pl.when(c == 3)
        def _():
            plane_pass(1)

        @pl.when(c == 4)
        def _():
            project(0, (3, 4))

        return carry

    lax.fori_loop(0, CHUNKS, enter, 0)

    row_start(4)
    plane_pass(2)
    row_end(3)
    plane_end(1)
    weights_ready(1)
    row_pass(4)
    row_start(5)

    def out_rows(quarter, start, size):
        base = pl.multiple_of(quarter * PART + start - HALO, 16)
        return pl.ds(start, size), pl.ds(base, size)

    def send_out(at, j, start, size):
        here, there = out_rows(mine, start, size)
        to = peer(j)
        return remote(
            hbuf.at[to, here], out.at[there], so.at[at, j], ro.at[at, me], (sp, 4 * half + to)
        )

    def keep_out(at, start, size):
        here, there = out_rows(mine, start, size)
        return pltpu.make_async_copy(hbuf.at[me, here], out.at[there], loc_o.at[at])

    def wait_out(at, j, start, size):
        frm = peer(j)
        _, there = out_rows((frm + 2 * half) % 4, start, size)
        ref = out.at[there]
        return remote(ref, ref, so.at[at, j], ro.at[at, frm], (sp, 4 * half + frm))

    mix_copy.wait()
    for l in range(LAYERS):
        last = l == LAYERS - 1
        if l == 1:
            row_end(5)
            plane_end(3)
            weights_ready(3)
        if l == 2:
            plane_end(5)
            weights_ready(5)

        def one(c, carry, l=l, last=last):
            s = l * CHUNKS + c
            on_x(l, c, s, lambda copy: copy.wait_recv())
            mix(l, c, s)
            if last:
                finish(c)
            else:
                share_squares(s + CHUNKS, update(l, c))

                if l == 0:

                    @pl.when(c == 1)
                    def _():
                        plane_end(2)

                    @pl.when(c == 3)
                    def _():
                        plane_pass(3)
                        row_pass(5)
                        row_end(4)

                else:

                    @pl.when(c == 0)
                    def _():
                        plane_pass(4)

                    @pl.when(c == 1)
                    def _():
                        plane_pass(5)

                @pl.when(c == 2)
                def _():
                    if l == 1:
                        plane_end(4)
                    weights_ready(2 * l + 2)
                    project(l + 1, (0, 1, 2))

                @pl.when(c == 4)
                def _():
                    project(l + 1, (3, 4))

            return carry

        lax.fori_loop(0, CHUNKS - 1 if last else CHUNKS, one, 0)

    end = CHUNKS - 1
    for n, (first, size) in enumerate(((0, SPLIT), (SPLIT, CH - SPLIT))):
        x_kept(LAYERS - 1, end, STEPS - 1)[n].wait_recv()
        mix(LAYERS - 1, end, STEPS - 1, first, size)
        finish(end, first, size)

    for m in range(MATS):
        c0(m).wait_send()
        for k, j in pairs:
            c1(m, k, j).wait_send()
            c1f(m, k, j).wait_send()
            for p in parts_of(m):
                c2(m, k, j, p).wait_send()
            c2f(m, k, j).wait_send()
        for k in range(2):
            for p in range(4):
                c3(m, k, p).wait_send()
    for j in range(1, 4):
        h_halo(j).wait_send()

    @pl.when(mine == 0)
    def _():
        labels().wait_send()
        h_halo(0).wait_send()

    for c in range(CHUNKS):
        for j in range(1, 4):
            h_main(c, j).wait_send()
    for l in range(LAYERS):
        for c in range(CHUNKS):
            s = l * CHUNKS + c
            for copy in x_kept(l, c, s):
                copy.wait_send()
            send_sq(s).wait_send()
    pieces = [(HALO, CH - HALO)] + [(c * CH, CH) for c in range(1, CHUNKS - 1)]
    pieces += [(end * CH, SPLIT), (end * CH + SPLIT, CH - SPLIT)]
    for at, (start, size) in enumerate(pieces):
        keep_out(at, start, size).wait()
        for j in range(1, 4):
            send_out(at, j, start, size).wait_send()
            wait_out(at, j, start, size).wait_recv()


def body(stream, doc_ids, norm_gain, proj_in, mix_pool, pool_gain, proj_out):
    dma = pltpu.SemaphoreType.DMA
    steps = STEPS
    vmem = pl.BlockSpec(memory_space=pltpu.VMEM)
    hbm = pl.BlockSpec(memory_space=pl.ANY)
    return pl.pallas_call(
        kernel,
        out_shape=pltpu.VMEM((TOK, COLS), BF16),
        in_specs=[hbm, vmem, vmem, hbm, hbm, hbm, vmem],
        out_specs=vmem,
        scratch_shapes=[
            pltpu.VMEM((MATS, 2, 2, 4, 4, 64, COLS), BF16),
            pltpu.VMEM((4, HALO + PART, COLS), BF16),
            pltpu.VMEM((steps, CH, POOL), BF16),
            pltpu.VMEM((steps, CH, POOL), BF16),
            pltpu.VMEM((steps, 8, 128), F32),
            pltpu.VMEM((steps, 8, 128), F32),
            pltpu.VMEM((CHUNKS * CH, WIDE), BF16),
            pltpu.VMEM((LEAD + CH, POOL), BF16),
            pltpu.VMEM((CH, POOL), BF16),
            pltpu.VMEM((128, 128), F32),
            pltpu.VMEM((CHUNKS, 4, CH, 128), BF16),
            pltpu.VMEM((CHUNKS, 4, CH, 128), F32),
            pltpu.VMEM((24, 128), jnp.int32),
            pltpu.VMEM((LAYERS, GROUPS, GROUP, GROUP), BF16),
            dma((MATS,)), dma((CHUNKS,)), dma((1,)), dma((CHUNKS + 1,)), dma((1,)),
            dma((MATS,)), dma((MATS,)),
            dma((MATS, 2, 2)), dma((MATS, 2, 2)), dma((MATS, 2, 2)), dma((MATS, 2, 2)),
            dma((MATS, 2, 2, 4)), dma((MATS, 2, 2, 4)), dma((MATS, 2, 2)), dma((MATS, 2, 2)),
            dma((MATS, 2, 4)), dma((MATS, 2, 4)),
            dma((CHUNKS, 4)), dma((CHUNKS, 4)), dma((4,)), dma((4,)), dma((1,)), dma((1,)),
            dma((steps + 5,)), dma((steps + 5,)), dma((steps,)), dma((steps,)),
            dma((CHUNKS + 1, 4)), dma((CHUNKS + 1, 4)),
        ],
        compiler_params=pltpu.CompilerParams(
            has_side_effects=True, collective_id=0, vmem_limit_bytes=56 * 1024 * 1024
        ),
        name="mixers",
    )(
        stream, doc_ids.reshape(16, 128), norm_gain, jnp.swapaxes(proj_in, 1, 2), proj_out,
        mix_pool, pool_gain,
    )


def solution(mesh):
    in_specs = (P("sp", "tp"), P("sp"), P(), P(None, "tp", "sp"), P(), P(), P(None, "sp", "tp"))
    out_specs = P("sp", "tp")
    return jax.shard_map(body, mesh=mesh, in_specs=in_specs, out_specs=out_specs, check_vma=False)
```

```python
import jax
import jax.numpy as jnp
from jax import lax
from jax.experimental import pallas as pl
from jax.experimental.pallas import tpu as pltpu
from jax.sharding import PartitionSpec as P

MESH = pl.DeviceIdType.MESH
F32 = jnp.float32
BF16 = jnp.bfloat16

D = 4096
POOL = 1024
GROUP = 128
GROUPS = POOL // GROUP
LAYERS = 3
MATS = 2 * LAYERS
TOK = 2048
COLS = 512
PART = TOK // 4
WIDE = 4 * COLS
HALO = 48
LEAD = 16
CHUNKS = 5
CH = (HALO + PART) // CHUNKS
WINDOWS = (2, 4, 8, 16)
STEPS = LAYERS * CHUNKS
SPLIT = 64
EPS = 1e-06


def kernel(
    stream, docs, norm_gain, w_in, w_out, mix_hbm, pool_gain, out,
    wbuf, hbuf, own, got, ssown, ssgot, gbuf, zbuf, mbuf, sqbuf, band, inv, ext, mix_pool,
    loc_w, loc_h, loc_hh, loc_o, loc_m,
    s0, r0, s1, r1, s1f, r1f, s2, r2, s2f, r2f, s3, r3,
    sh, rh, shh, rhh, sl, rl, sx, rx, sq, rq, so, ro,
):
    sp = lax.axis_index("sp")
    tp = lax.axis_index("tp")
    z, y = sp // 4, sp % 4
    x, core = tp // 2, tp % 2
    half, xl = x // 2, x % 2
    me = xl * 2 + core
    mine = (me + 2 * half) % 4

    def remote(src, dst, send, recv, device):
        return pltpu.make_async_remote_copy(
            src_ref=src, dst_ref=dst, send_sem=send, recv_sem=recv,
            device_id=device, device_id_type=MESH,
        )

    across = (sp, (2 * half + 1 - xl) * 2 + core)
    partner = (sp, (3 - x) * 2 + core)
    sibling = (sp, x * 2 + 1 - core)

    def along_y(d):
        return (z * 4 + (y + d + 4) % 4, tp)

    def along_z(d):
        return (((z + d + 4) % 4) * 4 + y, tp)

    first_axis = (along_y, along_z)
    second_axis = (along_z, along_y)
    steps = (1, -1)

    def shard(m, k, d):
        if k == 0:
            return wbuf.at[m, core, 0, z, (y + d + 4) % 4]
        return wbuf.at[m, core, 1, (z + d + 4) % 4, y]

    def plane(m, k, d, c=None):
        c = core if c is None else c
        if k == 0:
            return wbuf.at[m, c, 0, (z + d + 4) % 4]
        return wbuf.at[m, c, 1, :, (y + d + 4) % 4]

    def plane_half(m, k, d, which):
        part = pl.ds(2 * which, 2)
        if k == 0:
            return wbuf.at[m, core, 0, (z + d + 4) % 4, part]
        return wbuf.at[m, core, 1, part, (y + d + 4) % 4]

    pairs = [(k, j) for k in range(2) for j in range(2)]

    def c_local(m):
        source = w_in if m % 2 == 0 else w_out
        return pltpu.make_async_copy(source.at[m // 2], wbuf.at[m, core, xl, z, y], loc_w.at[m])

    def c0(m):
        return remote(wbuf.at[m, core, xl, z, y], wbuf.at[m, core, xl, z, y], s0.at[m], r0.at[m], across)

    def c1(m, k, j):
        return remote(shard(m, k, 0), shard(m, k, 0), s1.at[m, k, j], r1.at[m, k, j], first_axis[k](steps[j]))

    def c1f(m, k, j):
        ref = shard(m, k, -steps[j]).at[pl.ds(32 * j, 32)]
        return remote(ref, ref, s1f.at[m, k, j], r1f.at[m, k, j], first_axis[k](steps[j]))

    def c2(m, k, j, p):
        ref = shard(m, k, (0, -1, 1, 2)[p]) if m == 0 else plane(m, k, 0)
        return remote(ref, ref, s2.at[m, k, j, p], r2.at[m, k, j, p], second_axis[k](steps[j]))

    def c2f(m, k, j):
        ref = plane_half(m, k, -steps[j], j)
        return remote(ref, ref, s2f.at[m, k, j], r2f.at[m, k, j], second_axis[k](steps[j]))

    def c3(m, k, p):
        ref = plane(m, k, (0, -1, 1, 2)[p])
        return remote(ref, ref, s3.at[m, k, p], r3.at[m, k, p], sibling)

    def parts_of(m):
        return range(4 if m == 0 else 1)

    def row_start(m):
        c0(m).wait_recv()
        for k, j in pairs:
            c1(m, k, j).start()
        if m == 0:
            for k, j in pairs:
                c2(m, k, j, 0).start()

    def row_pass(m):
        for k, j in pairs:
            c1(m, k, j).wait_recv()
            c1f(m, k, j).start()
        if m == 0:
            for k, j in pairs:
                c2(m, k, 0, 1 + j).start()
                c2(m, k, 1, 1 + j).start()

    def row_end(m):
        for k in range(2):
            for j in range(2):
                c1f(m, k, j).wait_recv()
            for j in range(2):
                c2(m, k, j, 3 if m == 0 else 0).start()
            c3(m, k, 0).start()

    def plane_pass(m):
        for k, j in pairs:
            for p in parts_of(m):
                c2(m, k, j, p).wait_recv()
            c2f(m, k, j).start()
            c3(m, k, 1 + j).start()

    def plane_end(m):
        for k, j in pairs:
            c2f(m, k, j).wait_recv()
        for k in range(2):
            c3(m, k, 3).start()

    def weights_ready(m):
        for k in range(2):
            for p in range(4):
                c3(m, k, p).wait_recv()

    def peer(j):
        return (me + j) % 4

    def rows_of(c):
        return (HALO, CH - HALO) if c == 0 else (CH * c, CH)

    def h_main(c, j):
        to = peer(j)
        start, size = rows_of(c)
        base = ((to + 2 * half) % 4) * PART + start - HALO
        return remote(
            stream.at[pl.ds(pl.multiple_of(base, 16), size)], hbuf.at[me, pl.ds(start, size)],
            sh.at[c, j], rh.at[c, me], (sp, 4 * half + to),
        )

    def h_main_wait(c, j):
        start, size = rows_of(c)
        ref = hbuf.at[peer(j), pl.ds(start, size)]
        return remote(ref, ref, sh.at[c, j], rh.at[c, peer(j)], (sp, 4 * half + peer(j)))

    def h_main_local(c):
        start, size = rows_of(c)
        base = mine * PART + start - HALO
        return pltpu.make_async_copy(
            stream.at[pl.ds(pl.multiple_of(base, 16), size)], hbuf.at[me, pl.ds(start, size)], loc_h.at[c]
        )

    def h_halo(j):
        to = peer(j)
        quarter = (to + 2 * half) % 4
        base = (quarter * PART + TOK - HALO) % TOK
        to_sp = (sp + 1 - (quarter + 3) // 4) % 16
        return remote(
            stream.at[pl.ds(pl.multiple_of(base, 16), HALO)], hbuf.at[me, pl.ds(0, HALO)],
            shh.at[j], rhh.at[me], (to_sp, 4 * half + to),
        )

    def h_halo_wait(j):
        ref = hbuf.at[peer(j), pl.ds(0, HALO)]
        return remote(ref, ref, shh.at[j], rhh.at[peer(j)], (sp, 4 * half + peer(3)))

    def h_halo_local():
        base = (mine * PART + TOK - HALO) % TOK
        return pltpu.make_async_copy(
            stream.at[pl.ds(pl.multiple_of(base, 16), HALO)], hbuf.at[me, pl.ds(0, HALO)], loc_hh.at[0]
        )

    def labels():
        return remote(docs.at[pl.ds(15, 1)], ext.at[pl.ds(7, 1)], sl.at[0], rl.at[0], ((sp + 1) % 16, tp))

    mix_copy = pltpu.make_async_copy(mix_hbm, mix_pool, loc_m.at[0])
    for m in range(MATS):
        c_local(m).start()
    mix_copy.start()
    greeted = [across, partner, sibling, (sp, (2 * half + 1 - xl) * 2 + 1 - core)]
    greeted += [along_y(1), along_y(-1), along_z(1), along_z(-1)]
    barrier = pltpu.get_barrier_semaphore()
    for device in greeted:
        pl.semaphore_signal(barrier, inc=1, device_id=device, device_id_type=MESH)

    @pl.when(mine == 0)
    def _():
        for j in range(4):
            device = ((sp + 15) % 16, 4 * half + peer(j))
            pl.semaphore_signal(barrier, inc=1, device_id=device, device_id_type=MESH)

    pl.semaphore_wait(barrier, len(greeted) + 1)

    for m in range(3):
        c_local(m).wait()
        c0(m).start()
    for j in range(1, 4):
        h_halo(j).start()

    @pl.when(mine == 0)
    def _():
        labels().start()
        h_halo(0).start()

    @pl.when(mine != 0)
    def _():
        h_halo_local().start()

    for c in range(CHUNKS):
        h_main_local(c).start()
        for j in range(1, 4):
            h_main(c, j).start()
        if c == 2:
            for m in (3, 4):
                c_local(m).wait()
                c0(m).start()
    for m in range(5, MATS):
        c_local(m).wait()
        c0(m).start()

    row_start(0)

    zbuf[...] = jnp.zeros_like(zbuf)
    sqbuf[...] = jnp.zeros_like(sqbuf)
    for l in range(1, LAYERS):
        got[l * CHUNKS, 0 : LEAD * l, :] = jnp.zeros((LEAD * l, POOL), BF16)
    ext[8:24, :] = docs[...]

    @pl.when(mine == 0)
    def _():
        labels().wait_recv()

    label_rows = []
    for k in range(5):
        row = (ext[pl.ds(4 * mine + 7 + k, 1), :] + 1).astype(F32)
        if k == 0:
            row = jnp.where(jnp.logical_and(sp == 0, mine == 0), jnp.zeros_like(row), row)
        label_rows.append(row)
    t_id = lax.broadcasted_iota(jnp.int32, (128, 128), 0)
    s_id = lax.broadcasted_iota(jnp.int32, (128, 128), 1)
    back = t_id - s_id
    lane = lax.broadcasted_iota(jnp.int32, (1, 128), 1)
    for c in range(CHUNKS):
        first, off = divmod(128 - HALO - LEAD + CH * c, 128)
        if off == 0:
            window = label_rows[first]
        else:
            window = jnp.where(
                lane < 128 - off,
                pltpu.roll(label_rows[first], 128 - off, 1),
                pltpu.roll(label_rows[first + 1], 128 - off, 1),
            )
        across_lanes = jnp.broadcast_to(window, (128, 128))
        same = jnp.logical_and(across_lanes == across_lanes.T, back >= 0)
        for i, w in enumerate(WINDOWS):
            member = jnp.where(jnp.logical_and(same, back < w), 1.0, 0.0).astype(F32)
            count = jnp.sum(member, axis=1, keepdims=True)
            band[c, i] = member[LEAD:].astype(BF16)
            inv[c, i] = jnp.broadcast_to(1.0 / count, (128, 128))[LEAD:]

    row_pass(0)
    row_end(0)
    row_start(1)
    row_start(2)
    plane_pass(0)
    row_pass(1)
    row_pass(2)
    row_start(3)
    plane_end(0)
    row_end(1)
    weights_ready(0)
    row_end(2)

    def rows_at(c):
        return pl.ds(pl.multiple_of(c * CH, 16), CH)

    def squares_of(wide):
        total = None
        for k in range(COLS // 128):
            piece = wide[:, k * 128 : (k + 1) * 128]
            total = piece * piece if total is None else total + piece * piece
        return total

    def gain_of(l, b):
        at = pl.ds(pl.multiple_of(half * WIDE + b * COLS, COLS), COLS)
        return norm_gain[l : l + 1, at].astype(F32)

    def send_x(s, at, rows=(0, CH), lanes=(0, POOL)):
        index = (s, pl.ds(*rows), pl.ds(*lanes))
        return remote(own.at[index], got.at[index], sx.at[at], rx.at[at], partner)

    def x_first(n):
        return send_x(0, STEPS + 1 + n, lanes=(n * 256, 256))

    def x_kept(l, c, s):
        if c == 0 and l > 0:
            return [send_x(s, s, rows=(LEAD * l, CH - LEAD * l))]
        if c == CHUNKS - 1 and l == LAYERS - 1:
            return [send_x(s, s, rows=(0, SPLIT)), send_x(s, STEPS, rows=(SPLIT, CH - SPLIT))]
        if c == 0:
            return [x_first(n) for n in range(4)]
        return [send_x(s, s)]

    def on_x(l, c, s, act):
        special = [0, CHUNKS - 1] if l == LAYERS - 1 else [0]
        plain = c != 0
        for k in special:

            @pl.when(c == k)
            def _(k=k):
                for copy in x_kept(l, k, s):
                    act(copy)

            plain = jnp.logical_and(plain, c != k)

        @pl.when(plain)
        def _():
            act(send_x(s, s))

    def send_sq(s):
        return remote(ssown.at[s], ssgot.at[s], sq.at[s], rq.at[s], partner)

    def share_squares(s, squares):
        sqbuf[0:CH, :] = squares
        ssown[s] = jnp.broadcast_to(jnp.sum(sqbuf[...].T, axis=0, keepdims=True), (8, 128))
        send_sq(s).start()

    def project(l, chunks):
        rows = slice(chunks[0] * CH, (chunks[-1] + 1) * CH)
        for n in range(4):
            rhs = jnp.concatenate(
                [wbuf[2 * l, b % 2, b // 2, n].reshape(256, COLS) for b in range(4)], axis=1
            )
            part = lax.dot_general(
                gbuf[rows, :], rhs, (((1,), (1,)), ((), ())), preferred_element_type=F32
            ).astype(BF16)
            for k, c in enumerate(chunks):
                own[l * CHUNKS + c, :, n * 256 : (n + 1) * 256] = part[k * CH : (k + 1) * CH]
                if l == 0 and c == 0:
                    x_first(n).start()
        for c in chunks:
            if l > 0 or c > 0:
                for copy in x_kept(l, c, l * CHUNKS + c):
                    copy.start()

    def mix(l, c, s, first=0, size=CH):
        rows = slice(first, first + size)
        here = slice(LEAD + first, LEAD + first + size)
        if first == 0:
            send_sq(s).wait_recv()
            zbuf[0:LEAD, :] = zbuf[CH : CH + LEAD, :]
        scale = lax.rsqrt((ssown[s] + ssgot[s]) / D + EPS)[0:1]
        scale = jnp.broadcast_to(scale, (128, 128)).T[rows]
        for i in range(GROUPS):
            at = slice(i * GROUP, (i + 1) * GROUP)
            summed = own[s, rows, at].astype(F32) + got[s, rows, at].astype(F32)
            zbuf[here, at] = (summed * scale).astype(BF16)
        for i in range(GROUPS):
            at = slice(i * GROUP, (i + 1) * GROUP)
            total = jnp.dot(band[c, i % 4, rows], zbuf[:, at], preferred_element_type=F32)
            pooled = (total * inv[c, i % 4, rows] - zbuf[here, at].astype(F32)).astype(BF16)
            blended = jnp.dot(pooled, mix_pool[l, i], preferred_element_type=F32)
            mbuf[rows, at] = (blended * pool_gain[l : l + 1, at].astype(F32)).astype(BF16)

    def update(l, c):
        rows = rows_at(c)
        squares = None
        for b in range(4):
            weights = wbuf[2 * l + 1, b % 2, b // 2].reshape(POOL, COLS)
            change = jnp.dot(mbuf[...], weights, preferred_element_type=F32)
            new = (hbuf[b, rows, :].astype(F32) + change).astype(BF16)
            hbuf[b, rows, :] = new
            wide = new.astype(F32)
            squares = squares_of(wide) if squares is None else squares + squares_of(wide)
            gbuf[rows, b * COLS : (b + 1) * COLS] = (wide * gain_of(l + 1, b)).astype(BF16)
        return squares

    def finish(c, first=0, size=CH):
        for j in (2, 3, 1, 0):
            b = peer(j)
            weights = wbuf[MATS - 1, b % 2, b // 2].reshape(POOL, COLS)
            change = jnp.dot(mbuf[first : first + size], weights, preferred_element_type=F32)
            rows = pl.ds(pl.multiple_of(c * CH + first, 16), size)
            hbuf[b, rows, :] = (hbuf[b, rows, :].astype(F32) + change).astype(BF16)
            if isinstance(c, int):
                at = c + (first > 0)
                (send_out(at, j, c * CH + first, size) if j else keep_out(at, c * CH + first, size)).start()
                continue
            for start, size_ in ((HALO, CH - HALO), (pl.multiple_of(c * CH, 16), CH)):

                @pl.when(c == 0 if size_ < CH else c != 0)
                def _(j=j, start=start, size_=size_):
                    (send_out(c, j, start, size_) if j else keep_out(c, start, size_)).start()

    def wait_rows(c):
        h_main_local(c).wait()
        for j in range(1, 4):
            h_main_wait(c, j).wait_recv()

    @pl.when(mine == 0)
    def _():
        h_halo_wait(0).wait_recv()

    @pl.when(mine != 0)
    def _():
        h_halo_local().wait()

    for j in range(1, 4):
        h_halo_wait(j).wait_recv()

    def enter(c, carry):
        for k in range(CHUNKS):

            @pl.when(c == k)
            def _(k=k):
                wait_rows(k)

        rows = rows_at(c)
        squares = None
        for b in range(4):
            wide = hbuf[b, rows, :].astype(F32)
            squares = squares_of(wide) if squares is None else squares + squares_of(wide)
            gbuf[rows, b * COLS : (b + 1) * COLS] = (wide * gain_of(0, b)).astype(BF16)
        share_squares(c, squares)

        @pl.when(c == 1)
        def _():
            project(0, (0, 1))

        @pl.when(c == 2)
        def _():
            project(0, (2,))
            row_pass(3)

        @pl.when(c == 3)
        def _():
            plane_pass(1)

        @pl.when(c == 4)
        def _():
            project(0, (3, 4))

        return carry

    lax.fori_loop(0, CHUNKS, enter, 0)

    row_start(4)
    plane_pass(2)
    row_end(3)
    plane_end(1)
    weights_ready(1)
    row_pass(4)
    row_start(5)

    def out_rows(quarter, start, size):
        base = pl.multiple_of(quarter * PART + start - HALO, 16)
        return pl.ds(start, size), pl.ds(base, size)

    def send_out(at, j, start, size):
        here, there = out_rows(mine, start, size)
        to = peer(j)
        return remote(
            hbuf.at[to, here], out.at[there], so.at[at, j], ro.at[at, me], (sp, 4 * half + to)
        )

    def keep_out(at, start, size):
        here, there = out_rows(mine, start, size)
        return pltpu.make_async_copy(hbuf.at[me, here], out.at[there], loc_o.at[at])

    def wait_out(at, j, start, size):
        frm = peer(j)
        _, there = out_rows((frm + 2 * half) % 4, start, size)
        ref = out.at[there]
        return remote(ref, ref, so.at[at, j], ro.at[at, frm], (sp, 4 * half + frm))

    mix_copy.wait()
    for l in range(LAYERS):
        last = l == LAYERS - 1
        if l == 1:
            row_end(5)
            plane_end(3)
            weights_ready(3)
        if l == 2:
            plane_end(5)
            weights_ready(5)

        def one(c, carry, l=l, last=last):
            s = l * CHUNKS + c
            on_x(l, c, s, lambda copy: copy.wait_recv())
            mix(l, c, s)
            if last:
                finish(c)
            else:
                share_squares(s + CHUNKS, update(l, c))

                if l == 0:

                    @pl.when(c == 1)
                    def _():
                        plane_end(2)

                    @pl.when(c == 3)
                    def _():
                        plane_pass(3)
                        row_pass(5)
                        row_end(4)

                else:

                    @pl.when(c == 0)
                    def _():
                        plane_pass(4)

                    @pl.when(c == 1)
                    def _():
                        plane_pass(5)

                @pl.when(c == 2)
                def _():
                    if l == 1:
                        plane_end(4)
                    weights_ready(2 * l + 2)
                    project(l + 1, (0, 1, 2))

                @pl.when(c == 4)
                def _():
                    project(l + 1, (3, 4))

            return carry

        lax.fori_loop(0, CHUNKS - 1 if last else CHUNKS, one, 0)

    end = CHUNKS - 1
    for n, (first, size) in enumerate(((0, SPLIT), (SPLIT, CH - SPLIT))):
        x_kept(LAYERS - 1, end, STEPS - 1)[n].wait_recv()
        mix(LAYERS - 1, end, STEPS - 1, first, size)
        finish(end, first, size)

    for m in range(MATS):
        c0(m).wait_send()
        for k, j in pairs:
            c1(m, k, j).wait_send()
            c1f(m, k, j).wait_send()
            for p in parts_of(m):
                c2(m, k, j, p).wait_send()
            c2f(m, k, j).wait_send()
        for k in range(2):
            for p in range(4):
                c3(m, k, p).wait_send()
    for j in range(1, 4):
        h_halo(j).wait_send()

    @pl.when(mine == 0)
    def _():
        labels().wait_send()
        h_halo(0).wait_send()

    for c in range(CHUNKS):
        for j in range(1, 4):
            h_main(c, j).wait_send()
    for l in range(LAYERS):
        for c in range(CHUNKS):
            s = l * CHUNKS + c
            for copy in x_kept(l, c, s):
                copy.wait_send()
            send_sq(s).wait_send()
    pieces = [(HALO, CH - HALO)] + [(c * CH, CH) for c in range(1, CHUNKS - 1)]
    pieces += [(end * CH, SPLIT), (end * CH + SPLIT, CH - SPLIT)]
    for at, (start, size) in enumerate(pieces):
        keep_out(at, start, size).wait()
        for j in range(1, 4):
            send_out(at, j, start, size).wait_send()
            wait_out(at, j, start, size).wait_recv()


def body(stream, doc_ids, norm_gain, proj_in, mix_pool, pool_gain, proj_out):
    dma = pltpu.SemaphoreType.DMA
    steps = STEPS
    vmem = pl.BlockSpec(memory_space=pltpu.VMEM)
    hbm = pl.BlockSpec(memory_space=pl.ANY)
    return pl.pallas_call(
        kernel,
        out_shape=pltpu.VMEM((TOK, COLS), BF16),
        in_specs=[hbm, vmem, vmem, hbm, hbm, hbm, vmem],
        out_specs=vmem,
        scratch_shapes=[
            pltpu.VMEM((MATS, 2, 2, 4, 4, 64, COLS), BF16),
            pltpu.VMEM((4, HALO + PART, COLS), BF16),
            pltpu.VMEM((steps, CH, POOL), BF16),
            pltpu.VMEM((steps, CH, POOL), BF16),
            pltpu.VMEM((steps, 8, 128), F32),
            pltpu.VMEM((steps, 8, 128), F32),
            pltpu.VMEM((CHUNKS * CH, WIDE), BF16),
            pltpu.VMEM((LEAD + CH, POOL), BF16),
            pltpu.VMEM((CH, POOL), BF16),
            pltpu.VMEM((128, 128), F32),
            pltpu.VMEM((CHUNKS, 4, CH, 128), BF16),
            pltpu.VMEM((CHUNKS, 4, CH, 128), F32),
            pltpu.VMEM((24, 128), jnp.int32),
            pltpu.VMEM((LAYERS, GROUPS, GROUP, GROUP), BF16),
            dma((MATS,)), dma((CHUNKS,)), dma((1,)), dma((CHUNKS + 1,)), dma((1,)),
            dma((MATS,)), dma((MATS,)),
            dma((MATS, 2, 2)), dma((MATS, 2, 2)), dma((MATS, 2, 2)), dma((MATS, 2, 2)),
            dma((MATS, 2, 2, 4)), dma((MATS, 2, 2, 4)), dma((MATS, 2, 2)), dma((MATS, 2, 2)),
            dma((MATS, 2, 4)), dma((MATS, 2, 4)),
            dma((CHUNKS, 4)), dma((CHUNKS, 4)), dma((4,)), dma((4,)), dma((1,)), dma((1,)),
            dma((steps + 5,)), dma((steps + 5,)), dma((steps,)), dma((steps,)),
            dma((CHUNKS + 1, 4)), dma((CHUNKS + 1, 4)),
        ],
        compiler_params=pltpu.CompilerParams(
            has_side_effects=True, collective_id=0, vmem_limit_bytes=56 * 1024 * 1024
        ),
        name="mixers",
    )(
        stream, doc_ids.reshape(16, 128), norm_gain, jnp.swapaxes(proj_in, 1, 2), proj_out,
        mix_pool, pool_gain,
    )


def solution(mesh):
    in_specs = (P("sp", "tp"), P("sp"), P(), P(None, "tp", "sp"), P(), P(), P(None, "sp", "tp"))
    out_specs = P("sp", "tp")
    return jax.shard_map(body, mesh=mesh, in_specs=in_specs, out_specs=out_specs, check_vma=False)
```
